512 devices in a mesh: ep: 32 (over z, x), tp: 16 (over y, core).
Axes of the slice: x: 4, y: 8, z: 8, core: 2. Of those that a mesh axis runs over, the one named last changes fastest.
Arguments:
- tokens: bfloat16 [8192, 2048], P('ep', 'tp'), may hold values from -6 to 6
- row_ids: int32 [8192, 16], P('ep'), may hold values from 0 to 131071, as said below
- row_gates: float32 [8192, 16], P('ep'), may hold values from 0.02 to 0.5
- key_table: bfloat16 [131072, 2048], P('ep', 'tp'), may hold values from -0.125 to 0.125
- value_table: bfloat16 [131072, 2048], P('ep', 'tp'), may hold values from -14 to 14
- norm_gain: float32 [2048], P('tp'), may hold values from 0.1 to 1.9
Outputs:
- output: bfloat16 [8192, 2048], P('ep', 'tp')
The draws below stay inside these ranges and needn't reach their ends.
Inputs may be any that keep to these rules, and one draw needn't show every extreme that they name: `row_ids`: table row r belongs to index r // 4096 of ep. The 256 tokens of one index of ep choose at most 384 rows belonging to any one index, exactly 384 from some index, and at least one from every index.
All inputs are finite; a program needn't handle non-finite values.
Results may differ from the reference program's by a relative error of at most 0.0065.
Values may be sent and summed in bfloat16 or wider, within the bound.
No kernel may reach another device: no remote copies, remote signals or barrier semaphores. Data moves between devices by JAX's collectives and lax.ppermute only.
A program may use at most 64 MiB of HBM per device.

```python
import math
import jax
import jax.numpy as jnp
from jax import lax

D = 2048
PICKS = 16
EXP_DEV = 4096
TOK_DEV = 256
EXPERTS = 131072
TOKENS = 8192
CAP = 384


def draw_row_ids(key, part):
    devices = TOKENS // TOK_DEV
    per_device = TOK_DEV * PICKS
    key_hot, key_order, key_local = jax.random.split(key, 3)
    hottest = jax.random.randint(key_hot, (devices, 1), 0, devices)
    slot = jnp.arange(per_device, dtype=jnp.int32)[None, :]
    spread = (slot - CAP) % (devices - 1)
    others = spread + (spread >= hottest).astype(jnp.int32)
    owner = jnp.where(slot < CAP, hottest, others)
    local = jax.random.randint(key_local, (devices, per_device), 0, EXP_DEV)
    order = jax.vmap(lambda k: jax.random.permutation(k, per_device))(jax.random.split(key_order, devices))
    chosen = jnp.take_along_axis(owner * EXP_DEV + local, order.astype(jnp.int32), axis=1)
    return chosen.reshape(TOKENS, PICKS).astype(jnp.int32)


def draw_value_table(key, part):
    key_base, key_rough = jax.random.split(key)
    column = jnp.arange(D, dtype=jnp.float32) / D
    rough = jax.random.uniform(key_rough, (D,), jnp.float32, 0.5, 1.5)
    base = jnp.clip(jax.random.normal(key_base, (EXPERTS, D), jnp.float32), -4.5, 4.5)
    rising = jnp.exp(math.log(4.0) * column)
    return (base * rising * rough * PICKS ** (-0.5)).astype(jnp.bfloat16)


def levels(stream_key, shape, pieces, least, high):
    level = 1.0
    for axis_at, blocks in pieces:
        steps = jax.random.uniform(jax.random.fold_in(jax.random.fold_in(stream_key, 6), axis_at), (blocks,), jnp.float32, least / len(pieces), high / len(pieces))
        level = level * jnp.repeat(jnp.exp(steps), shape[axis_at] // blocks).reshape((-1,) + (1,) * (len(shape) - 1 - axis_at))
    return level


def noise(key, dims, width, reach, pieces=(), held_as=jnp.bfloat16):
    array = width * jax.random.normal(key, dims, jnp.float32)
    if pieces:
        array = array * levels(key, dims, pieces, -0.22, 0.18)
    return jnp.clip(array, -reach, reach).astype(held_as)


def setup_inputs(seed: int = 0) -> dict:
    streams_of = jax.random.split(jax.random.key(seed), 7)
    return {
        "tokens": noise(streams_of[0], (TOKENS, D), 1.0, 6.0, ((0, 32), (1, 16))),
        "row_ids": draw_row_ids(jax.random.fold_in(streams_of[6], 71), 0),
        "row_gates": jnp.clip(jnp.exp(math.log(0.5) - 3.218876 * jax.random.uniform(streams_of[2], (TOKENS, PICKS), jnp.float32) ** levels(streams_of[2], (TOKENS, PICKS), ((0, 32),), -0.2, 0.2)), 0.02, 0.5),
        "key_table": noise(streams_of[3], (EXPERTS, D), D ** -0.5, 0.125, ((0, 32), (1, 16))),
        "value_table": draw_value_table(jax.random.fold_in(streams_of[6], 71), 0),
        "norm_gain": jnp.clip(1.0 + 0.18 * jax.random.normal(streams_of[5], (D,), jnp.float32), 0.1, 1.9),
    }


def reference(tokens, row_ids, row_gates, key_table, value_table, norm_gain):
    blocks = TOKENS // TOK_DEV

    def one_block(args):
        vectors, chosen, weights = args
        keys = key_table[chosen].astype(jnp.float32)
        score = jnp.einsum('td,tkd->tk', vectors.astype(jnp.float32), keys)
        hidden = jax.nn.gelu(score, approximate=False) * weights
        values = value_table[chosen].astype(jnp.float32)
        return jnp.einsum('tk,tkd->td', hidden, values)
    mixed = lax.map(one_block, (tokens.reshape(blocks, TOK_DEV, D), row_ids.reshape(blocks, TOK_DEV, PICKS), row_gates.reshape(blocks, TOK_DEV, PICKS)))
    mixed = mixed.reshape(TOKENS, D)
    strength = lax.optimization_barrier(jnp.mean(mixed * mixed, axis=-1, keepdims=True))
    return (mixed * lax.rsqrt(strength + 1e-06) * norm_gain).astype(jnp.bfloat16)
```

```python
import jax
import jax.numpy as jnp
from jax import lax
from jax.experimental import pallas as pl
from jax.experimental.pallas import tpu as pltpu
from jax.sharding import PartitionSpec as P

D = 2048
LANES = 128
INTERPRET = False


def bucket_kernel(ids_ref, gates_ref, out_ref, a_ref, b_ref, *, n_ep, cap, shift):
    picks, tok = ids_ref.shape
    before = jnp.where(
        lax.broadcasted_iota(jnp.int32, (tok, tok), 0)
        < lax.broadcasted_iota(jnp.int32, (tok, tok), 1),
        1.0,
        0.0,
    ).astype(jnp.bfloat16)
    token_no = (lax.broadcasted_iota(jnp.int32, (1, tok), 1) + 1).astype(jnp.float32)
    owners = lax.broadcasted_iota(jnp.int32, (n_ep, tok), 0)
    slots = lax.broadcasted_iota(jnp.int32, (cap, tok), 0)
    base = jnp.zeros((n_ep, 1), jnp.float32)
    for k in range(picks):
        ids = ids_ref[k : k + 1, :]
        mine = (ids >> shift) == owners
        hot = jnp.where(mine, 1.0, 0.0)
        rank = base + jnp.dot(
            hot.astype(jnp.bfloat16), before, preferred_element_type=jnp.float32
        )
        place = jnp.sum(jnp.where(mine, rank, 0.0), axis=0, keepdims=True).astype(jnp.int32)
        base = base + jnp.sum(hot, axis=1, keepdims=True)
        b_ref[:, k * tok : (k + 1) * tok] = jnp.where(slots == place, 1.0, 0.0).astype(
            jnp.bfloat16
        )
        local = ids & ((1 << shift) - 1)
        gate = gates_ref[k : k + 1, :]
        gate_hi = gate.astype(jnp.bfloat16).astype(jnp.float32)
        gate_mid = (gate - gate_hi).astype(jnp.bfloat16).astype(jnp.float32)
        gate_lo = gate - gate_hi - gate_mid
        values = (
            token_no,
            (local >> 4).astype(jnp.float32),
            (local & 15).astype(jnp.float32),
            gate_hi,
            gate_mid,
            gate_lo,
        )
        for c, value in enumerate(values):
            a_ref[c * n_ep : (c + 1) * n_ep, k * tok : (k + 1) * tok] = jnp.where(
                mine, value, 0.0
            ).astype(jnp.bfloat16)
    res = lax.dot_general(
        a_ref[...], b_ref[...], (((1,), (1,)), ((), ())), preferred_element_type=jnp.float32
    )
    part = [res[c * n_ep : (c + 1) * n_ep] for c in range(6)]
    code = part[0] * float(1 << shift) + (part[1] * 16.0 + part[2])
    gates = part[3] + part[4] + part[5]
    chunks = cap // LANES
    out_ref[...] = jnp.zeros(out_ref.shape, jnp.float32)
    for j in range(chunks):
        out_ref[:, j, :] = code[:, j * LANES : (j + 1) * LANES]
        out_ref[:, chunks + j, :] = gates[:, j * LANES : (j + 1) * LANES]


def widen(table_ref, wide_ref):
    step = 256

    def one(i, carry):
        rows = pl.ds(pl.multiple_of(i * step, step), step)
        wide_ref[rows, :] = table_ref[rows, :].astype(jnp.float32)
        return carry

    lax.fori_loop(0, table_ref.shape[0] // step, one, 0)


def take_rows(rows_ref, line, wide_ref, rows_out):
    for s in range(LANES):
        rows_out[pl.ds(s, 1), :] = wide_ref[pl.ds(rows_ref[line, s], 1), :]


def score_kernel(rows_ref, count_ref, place_ref, tok_ref, key_ref, out_ref, wide, picked):
    n_ep, tok, _ = tok_ref.shape
    chunks = place_ref.shape[0] // n_ep
    widen(key_ref, wide)
    out_ref[...] = jnp.zeros(out_ref.shape, jnp.float32)
    token_of = lax.broadcasted_iota(jnp.int32, (tok, LANES), 0)

    def block(i, carry):
        def chunk(c, inner):
            line = i * chunks + c
            take_rows(rows_ref, line, wide, picked)
            prod = lax.dot_general(
                tok_ref[i],
                picked[...].astype(jnp.bfloat16),
                (((1,), (1,)), ((), ())),
                preferred_element_type=jnp.float32,
            )
            here = place_ref[pl.ds(line, 1), :] == token_of
            out_ref[pl.ds(line, 1), :] = jnp.sum(
                jnp.where(here, prod, 0.0), axis=0, keepdims=True
            )
            return inner

        return lax.fori_loop(0, (count_ref[i] + LANES - 1) // LANES, chunk, carry)

    lax.fori_loop(0, n_ep, block, 0)


def combine_kernel(rows_ref, count_ref, place_ref, hidden_ref, value_ref, out_ref, wide, picked, acc):
    n_ep, tok, _ = out_ref.shape
    chunks = place_ref.shape[0] // n_ep
    widen(value_ref, wide)
    token_of = lax.broadcasted_iota(jnp.int32, (tok, LANES), 0)

    def block(i, carry):
        acc[...] = jnp.zeros(acc.shape, jnp.float32)

        def chunk(c, inner):
            line = i * chunks + c
            take_rows(rows_ref, line, wide, picked)
            here = place_ref[pl.ds(line, 1), :] == token_of
            weight = jnp.where(here, hidden_ref[pl.ds(line, 1), :], 0.0)
            high = weight.astype(jnp.bfloat16)
            low = (weight - high.astype(jnp.float32)).astype(jnp.bfloat16)
            rows = picked[...].astype(jnp.bfloat16)
            acc[...] += jnp.dot(high, rows, preferred_element_type=jnp.float32) + jnp.dot(
                low, rows, preferred_element_type=jnp.float32
            )
            return inner

        lax.fori_loop(0, (count_ref[i] + LANES - 1) // LANES, chunk, 0)
        out_ref[i] = acc[...].astype(out_ref.dtype)
        return carry

    lax.fori_loop(0, n_ep, block, 0)


def vmem():
    return pl.BlockSpec(memory_space=pltpu.VMEM)


def smem():
    return pl.BlockSpec(memory_space=pltpu.SMEM)


def body(tokens, row_ids, row_gates, key_table, value_table, norm_gain):
    tok, width = tokens.shape
    picks = row_ids.shape[1]
    exp_dev = key_table.shape[0]
    n_ep = lax.axis_size("ep")
    cap = 3 * tok * picks // n_ep
    chunks = cap // LANES
    shift = exp_dev.bit_length() - 1
    lines = n_ep * chunks

    spread = lax.all_to_all(
        jnp.broadcast_to(tokens[None], (n_ep, tok, width)), "ep", 0, 0, tiled=True
    )
    listed = pl.pallas_call(
        lambda *refs: bucket_kernel(*refs, n_ep=n_ep, cap=cap, shift=shift),
        out_shape=jax.ShapeDtypeStruct((n_ep, 8, LANES), jnp.float32),
        in_specs=[vmem(), vmem()],
        out_specs=vmem(),
        scratch_shapes=[
            pltpu.VMEM((6 * n_ep, tok * picks), jnp.bfloat16),
            pltpu.VMEM((cap, tok * picks), jnp.bfloat16),
        ],
        interpret=INTERPRET,
        name="bucket",
    )(row_ids.T, row_gates.T)
    listed = lax.all_to_all(listed, "ep", 0, 0, tiled=True)
    codes = listed[:, :chunks].astype(jnp.int32)
    gates = listed[:, chunks : 2 * chunks].reshape(lines, LANES)
    rows = (codes & (exp_dev - 1)).reshape(lines, LANES)
    place = ((codes >> shift) - 1).reshape(lines, LANES)
    count = jnp.sum((codes > 0).astype(jnp.int32), axis=(1, 2))

    partial_score = pl.pallas_call(
        score_kernel,
        out_shape=jax.ShapeDtypeStruct((lines, LANES), jnp.float32),
        in_specs=[smem(), smem(), vmem(), vmem(), vmem()],
        out_specs=vmem(),
        scratch_shapes=[
            pltpu.VMEM((exp_dev, width), jnp.float32),
            pltpu.VMEM((LANES, width), jnp.float32),
        ],
        interpret=INTERPRET,
        name="score",
    )(rows, count, place, spread, key_table)
    score = jnp.sum(lax.all_gather(partial_score, "tp"), axis=0)
    hidden = jnp.where(place >= 0, jax.nn.gelu(score, approximate=False) * gates, 0.0)
    mixed_part = pl.pallas_call(
        combine_kernel,
        out_shape=jax.ShapeDtypeStruct((n_ep, tok, width), jnp.bfloat16),
        in_specs=[smem(), smem(), vmem(), vmem(), vmem()],
        out_specs=vmem(),
        scratch_shapes=[
            pltpu.VMEM((exp_dev, width), jnp.float32),
            pltpu.VMEM((LANES, width), jnp.float32),
            pltpu.VMEM((tok, width), jnp.float32),
        ],
        interpret=INTERPRET,
        name="combine",
    )(rows, count, place, hidden, value_table)
    back = lax.all_to_all(mixed_part, "ep", 0, 0, tiled=True)
    mixed = jnp.sum(back.astype(jnp.float32), axis=0)
    squares = jnp.sum(lax.all_gather(jnp.sum(mixed * mixed, axis=1), "tp"), axis=0)
    strength = squares / D
    return (mixed * lax.rsqrt(strength + 1e-06)[:, None] * norm_gain).astype(jnp.bfloat16)


def solution(mesh):
    in_specs = (P("ep", "tp"), P("ep", None), P("ep", None), P("ep", "tp"), P("ep", "tp"), P("tp"))
    out_specs = P("ep", "tp")
    return jax.shard_map(body, mesh=mesh, in_specs=in_specs, out_specs=out_specs, check_vma=False)
```

```python
import jax
import jax.numpy as jnp
from jax import lax
from jax.experimental import pallas as pl
from jax.experimental.pallas import tpu as pltpu
from jax.sharding import Mesh
from jax.sharding import PartitionSpec as P

D = 2048
LANES = 128
INTERPRET = False
Z = 8
EP = ("z", "x")
TP = ("y", "core")


def bucket_kernel(ids_ref, gates_ref, out_ref, a_ref, b_ref, *, n_ep, cap, shift):
    picks, tok = ids_ref.shape
    before = jnp.where(
        lax.broadcasted_iota(jnp.int32, (tok, tok), 0)
        < lax.broadcasted_iota(jnp.int32, (tok, tok), 1),
        1.0,
        0.0,
    ).astype(jnp.bfloat16)
    token_no = (lax.broadcasted_iota(jnp.int32, (1, tok), 1) + 1).astype(jnp.float32)
    owners = lax.broadcasted_iota(jnp.int32, (n_ep, tok), 0)
    slots = lax.broadcasted_iota(jnp.int32, (cap, tok), 0)
    base = jnp.zeros((n_ep, 1), jnp.float32)
    for k in range(picks):
        ids = ids_ref[k : k + 1, :]
        mine = (ids >> shift) == owners
        hot = jnp.where(mine, 1.0, 0.0)
        rank = base + jnp.dot(
            hot.astype(jnp.bfloat16), before, preferred_element_type=jnp.float32
        )
        place = jnp.sum(jnp.where(mine, rank, 0.0), axis=0, keepdims=True).astype(jnp.int32)
        base = base + jnp.sum(hot, axis=1, keepdims=True)
        b_ref[:, k * tok : (k + 1) * tok] = jnp.where(slots == place, 1.0, 0.0).astype(
            jnp.bfloat16
        )
        local = ids & ((1 << shift) - 1)
        gate = gates_ref[k : k + 1, :]
        gate_hi = gate.astype(jnp.bfloat16).astype(jnp.float32)
        gate_mid = (gate - gate_hi).astype(jnp.bfloat16).astype(jnp.float32)
        gate_lo = gate - gate_hi - gate_mid
        values = (
            token_no,
            (local >> 4).astype(jnp.float32),
            (local & 15).astype(jnp.float32),
            gate_hi,
            gate_mid,
            gate_lo,
        )
        for c, value in enumerate(values):
            a_ref[c * n_ep : (c + 1) * n_ep, k * tok : (k + 1) * tok] = jnp.where(
                mine, value, 0.0
            ).astype(jnp.bfloat16)
    res = lax.dot_general(
        a_ref[...], b_ref[...], (((1,), (1,)), ((), ())), preferred_element_type=jnp.float32
    )
    part = [res[c * n_ep : (c + 1) * n_ep] for c in range(6)]
    code = part[0] * float(1 << shift) + (part[1] * 16.0 + part[2])
    gates = part[3] + part[4] + part[5]
    chunks = cap // LANES
    out_ref[...] = jnp.zeros(out_ref.shape, jnp.float32)
    for j in range(chunks):
        out_ref[:, j, :] = code[:, j * LANES : (j + 1) * LANES]
        out_ref[:, chunks + j, :] = gates[:, j * LANES : (j + 1) * LANES]


def widen(table_ref, wide_ref):
    step = 256

    def one(i, carry):
        rows = pl.ds(pl.multiple_of(i * step, step), step)
        wide_ref[rows, :] = table_ref[rows, :].astype(jnp.float32)
        return carry

    lax.fori_loop(0, table_ref.shape[0] // step, one, 0)


def take_rows(rows_ref, line, wide_ref, picked, out_ref):
    for s in range(LANES):
        picked[pl.ds(s, 1), :] = wide_ref[pl.ds(rows_ref[line, s], 1), :]
    out_ref[line] = picked[...].astype(out_ref.dtype)


def each_line(count_ref, chunks, start, work, finish):
    def block(i, carry):
        start(i)

        def chunk(c, inner):
            work(i, i * chunks + c)
            return inner

        lax.fori_loop(0, (count_ref[i] + LANES - 1) // LANES, chunk, 0)
        finish(i)
        return carry

    lax.fori_loop(0, count_ref.shape[0], block, 0)


def nothing(i):
    del i


def pick_kernel(
    rows_ref, count_ref, key_ref, value_ref, keys_out, values_out, wide_k, wide_v, took_k, took_v
):
    widen(key_ref, wide_k)
    widen(value_ref, wide_v)
    chunks = keys_out.shape[0] // count_ref.shape[0]

    def work(i, line):
        take_rows(rows_ref, line, wide_k, took_k, keys_out)
        take_rows(rows_ref, line, wide_v, took_v, values_out)

    each_line(count_ref, chunks, nothing, work, nothing)


def score_kernel(count_ref, place_ref, tok_ref, keys_ref, out_ref):
    n_x, n_z, tok, _ = tok_ref.shape
    chunks = place_ref.shape[0] // (n_x * n_z)
    out_ref[...] = jnp.zeros(out_ref.shape, jnp.float32)
    token_of = lax.broadcasted_iota(jnp.int32, (tok, LANES), 0)

    def work(i, line):
        prod = lax.dot_general(
            tok_ref[i % n_x, i // n_x],
            keys_ref[line],
            (((1,), (1,)), ((), ())),
            preferred_element_type=jnp.float32,
        )
        here = place_ref[pl.ds(line, 1), :] == token_of
        out_ref[pl.ds(line, 1), :] = jnp.sum(jnp.where(here, prod, 0.0), axis=0, keepdims=True)

    each_line(count_ref, chunks, nothing, work, nothing)


def combine_kernel(count_ref, place_ref, hidden_ref, values_ref, out_ref, acc):
    n_ep, tok, _ = out_ref.shape
    chunks = place_ref.shape[0] // n_ep
    token_of = lax.broadcasted_iota(jnp.int32, (tok, LANES), 0)

    def start(i):
        acc[...] = jnp.zeros(acc.shape, jnp.float32)

    def work(i, line):
        here = place_ref[pl.ds(line, 1), :] == token_of
        weight = jnp.where(here, hidden_ref[pl.ds(line, 1), :], 0.0)
        high = weight.astype(jnp.bfloat16)
        low = (weight - high.astype(jnp.float32)).astype(jnp.bfloat16)
        rows = values_ref[line]
        acc[...] += jnp.dot(high, rows, preferred_element_type=jnp.float32) + jnp.dot(
            low, rows, preferred_element_type=jnp.float32
        )

    def finish(i):
        out_ref[i] = acc[...].astype(out_ref.dtype)

    each_line(count_ref, chunks, start, work, finish)


def vmem():
    return pl.BlockSpec(memory_space=pltpu.VMEM)


def smem():
    return pl.BlockSpec(memory_space=pltpu.SMEM)


def to_each(value, axis):
    return lax.all_to_all(
        jnp.broadcast_to(value[None], (lax.axis_size(axis), *value.shape)), axis, 0, 0, tiled=True
    )


def body(tokens, row_ids, row_gates, key_table, value_table, norm_gain):
    tok, width = tokens.shape
    picks = row_ids.shape[1]
    exp_dev = key_table.shape[0]
    n_ep = lax.axis_size(EP)
    cap = 3 * tok * picks // n_ep
    chunks = cap // LANES
    shift = exp_dev.bit_length() - 1
    lines = n_ep * chunks

    spread = to_each(to_each(tokens, "z"), "x")
    listed = pl.pallas_call(
        lambda *refs: bucket_kernel(*refs, n_ep=n_ep, cap=cap, shift=shift),
        out_shape=jax.ShapeDtypeStruct((n_ep, 8, LANES), jnp.float32),
        in_specs=[vmem(), vmem()],
        out_specs=vmem(),
        scratch_shapes=[
            pltpu.VMEM((6 * n_ep, tok * picks), jnp.bfloat16),
            pltpu.VMEM((cap, tok * picks), jnp.bfloat16),
        ],
        interpret=INTERPRET,
        name="bucket",
    )(row_ids.T, row_gates.T)
    listed = lax.all_to_all(listed, EP, 0, 0, tiled=True)
    codes = listed[:, :chunks].astype(jnp.int32)
    gates = listed[:, chunks : 2 * chunks].reshape(lines, LANES)
    rows = (codes & (exp_dev - 1)).reshape(lines, LANES)
    place = ((codes >> shift) - 1).reshape(lines, LANES)
    count = jnp.sum((codes > 0).astype(jnp.int32), axis=(1, 2))

    picked = jax.ShapeDtypeStruct((lines, LANES, width), jnp.bfloat16)
    keys, values = pl.pallas_call(
        pick_kernel,
        out_shape=(picked, picked),
        in_specs=[smem(), smem(), vmem(), vmem()],
        out_specs=(vmem(), vmem()),
        scratch_shapes=[
            pltpu.VMEM((exp_dev, width), jnp.float32),
            pltpu.VMEM((exp_dev, width), jnp.float32),
            pltpu.VMEM((LANES, width), jnp.float32),
            pltpu.VMEM((LANES, width), jnp.float32),
        ],
        interpret=INTERPRET,
        name="pick",
    )(rows, count, key_table, value_table)
    partial_score = pl.pallas_call(
        score_kernel,
        out_shape=jax.ShapeDtypeStruct((lines, LANES), jnp.float32),
        in_specs=[smem(), vmem(), vmem(), vmem()],
        out_specs=vmem(),
        interpret=INTERPRET,
        name="score",
    )(count, place, spread, keys)
    score = jnp.sum(lax.all_gather(partial_score, TP), axis=0)
    hidden = jnp.where(place >= 0, jax.nn.gelu(score, approximate=False) * gates, 0.0)
    mixed_part = pl.pallas_call(
        combine_kernel,
        out_shape=jax.ShapeDtypeStruct((n_ep, tok, width), jnp.bfloat16),
        in_specs=[smem(), vmem(), vmem(), vmem()],
        out_specs=vmem(),
        scratch_shapes=[pltpu.VMEM((tok, width), jnp.float32)],
        interpret=INTERPRET,
        name="combine",
    )(count, place, hidden, values)
    back = lax.all_to_all(mixed_part, EP, 0, 0, tiled=True)
    mixed = jnp.sum(back.astype(jnp.float32), axis=0)
    part = jnp.sum(mixed * mixed, axis=1).reshape(tok // LANES, LANES)
    squares = jnp.sum(to_each(part, TP), axis=0).reshape(tok)
    strength = squares / D
    return (mixed * lax.rsqrt(strength + 1e-06)[:, None] * norm_gain).astype(jnp.bfloat16)


def solution(mesh):
    ep, tp = mesh.devices.shape
    fine = Mesh(mesh.devices.reshape(Z, ep // Z, tp // 2, 2), ("z", "x", "y", "core"))
    in_specs = (P(EP, TP), P(EP, None), P(EP, None), P(EP, TP), P(EP, TP), P(TP))
    return jax.shard_map(body, mesh=fine, in_specs=in_specs, out_specs=P(EP, TP), check_vma=False)
```

```python
import jax
import jax.numpy as jnp
from jax import lax
from jax.experimental import pallas as pl
from jax.experimental.pallas import tpu as pltpu
from jax.sharding import Mesh
from jax.sharding import PartitionSpec as P

D = 2048
LANES = 128
INTERPRET = False
Z = 8
X = 4
SHIFTS = (0, 2, 1, 3)
EP = ("z", "x")
TP = ("y", "core")


def bucket_kernel(ids_ref, gates_ref, out_ref, a_ref, b_ref, *, n_ep, cap, shift):
    picks, tok = ids_ref.shape
    before = jnp.where(
        lax.broadcasted_iota(jnp.int32, (tok, tok), 0)
        < lax.broadcasted_iota(jnp.int32, (tok, tok), 1),
        1.0,
        0.0,
    ).astype(jnp.bfloat16)
    token_no = (lax.broadcasted_iota(jnp.int32, (1, tok), 1) + 1).astype(jnp.float32)
    owners = lax.broadcasted_iota(jnp.int32, (n_ep, tok), 0)
    slots = lax.broadcasted_iota(jnp.int32, (cap, tok), 0)
    base = jnp.zeros((n_ep, 1), jnp.float32)
    for k in range(picks):
        ids = ids_ref[k : k + 1, :]
        mine = (ids >> shift) == owners
        hot = jnp.where(mine, 1.0, 0.0)
        rank = base + jnp.dot(
            hot.astype(jnp.bfloat16), before, preferred_element_type=jnp.float32
        )
        place = jnp.sum(jnp.where(mine, rank, 0.0), axis=0, keepdims=True).astype(jnp.int32)
        base = base + jnp.sum(hot, axis=1, keepdims=True)
        b_ref[:, k * tok : (k + 1) * tok] = jnp.where(slots == place, 1.0, 0.0).astype(
            jnp.bfloat16
        )
        local = ids & ((1 << shift) - 1)
        gate = gates_ref[k : k + 1, :]
        gate_hi = gate.astype(jnp.bfloat16).astype(jnp.float32)
        gate_mid = (gate - gate_hi).astype(jnp.bfloat16).astype(jnp.float32)
        gate_lo = gate - gate_hi - gate_mid
        values = (
            token_no,
            (local >> 4).astype(jnp.float32),
            (local & 15).astype(jnp.float32),
            gate_hi,
            gate_mid,
            gate_lo,
        )
        for c, value in enumerate(values):
            a_ref[c * n_ep : (c + 1) * n_ep, k * tok : (k + 1) * tok] = jnp.where(
                mine, value, 0.0
            ).astype(jnp.bfloat16)
    res = lax.dot_general(
        a_ref[...], b_ref[...], (((1,), (1,)), ((), ())), preferred_element_type=jnp.float32
    )
    part = [res[c * n_ep : (c + 1) * n_ep] for c in range(6)]
    code = part[0] * float(1 << shift) + (part[1] * 16.0 + part[2])
    gates = part[3] + part[4] + part[5]
    chunks = cap // LANES
    out_ref[...] = jnp.zeros(out_ref.shape, jnp.float32)
    for j in range(chunks):
        out_ref[:, j, :] = code[:, j * LANES : (j + 1) * LANES]
        out_ref[:, chunks + j, :] = gates[:, j * LANES : (j + 1) * LANES]


def widen(table_ref, wide_ref):
    step = 256

    def one(i, carry):
        rows = pl.ds(pl.multiple_of(i * step, step), step)
        wide_ref[rows, :] = table_ref[rows, :].astype(jnp.float32)
        return carry

    lax.fori_loop(0, table_ref.shape[0] // step, one, 0)


def take_rows(rows_ref, line, wide_ref, picked, out_ref, to):
    for s in range(LANES):
        picked[pl.ds(s, 1), :] = wide_ref[pl.ds(rows_ref[line, s], 1), :]
    out_ref[to] = picked[...].astype(out_ref.dtype)


def chunks_of(count):
    return (count + LANES - 1) // LANES


def pick_kernel(
    x_ref,
    rows_ref,
    count_ref,
    place_ref,
    gate_ref,
    key_ref,
    value_ref,
    count_out,
    place_out,
    gate_out,
    keys_out,
    values_out,
    wide_k,
    wide_v,
    took_k,
    took_v,
):
    n_ep = count_ref.shape[0]
    n_z = n_ep // X
    chunks = place_ref.shape[0] // n_ep
    widen(key_ref, wide_k)
    widen(value_ref, wide_v)

    def block(i, carry):
        z = i // X
        shift = (x_ref[0] + X - i % X) % X
        slot = (shift // 2 + (shift % 2) * 2) * n_z + z
        count_out[slot] = count_ref[i]
        for c in range(chunks):
            place_out[pl.ds(slot * chunks + c, 1), :] = place_ref[pl.ds(i * chunks + c, 1), :]
            gate_out[pl.ds(slot * chunks + c, 1), :] = gate_ref[pl.ds(i * chunks + c, 1), :]

        def chunk(c, inner):
            take_rows(rows_ref, i * chunks + c, wide_k, took_k, keys_out, slot * chunks + c)
            take_rows(rows_ref, i * chunks + c, wide_v, took_v, values_out, slot * chunks + c)
            return inner

        lax.fori_loop(0, chunks_of(count_ref[i]), chunk, 0)
        return carry

    lax.fori_loop(0, n_ep, block, 0)


def score_kernel(count_ref, place_ref, keys_ref, tok0, tok1, tok2, tok3, out_ref):
    toks = (tok0, tok1, tok2, tok3)
    n_z, tok, _ = tok0.shape
    chunks = place_ref.shape[0] // (X * n_z)
    out_ref[...] = jnp.zeros(out_ref.shape, jnp.float32)
    token_of = lax.broadcasted_iota(jnp.int32, (tok, LANES), 0)

    def line_scores(tokens, line):
        prod = lax.dot_general(
            tokens, keys_ref[line], (((1,), (1,)), ((), ())), preferred_element_type=jnp.float32
        )
        here = place_ref[pl.ds(line, 1), :] == token_of
        return jnp.sum(jnp.where(here, prod, 0.0), axis=0, keepdims=True)

    def first(z, carry):
        lines = [(g * n_z + z) * chunks for g in range(X)]
        found = [line_scores(toks[g][z], lines[g]) for g in range(X)]
        for line, value in zip(lines, found):
            out_ref[pl.ds(line, 1), :] = value
        return carry

    lax.fori_loop(0, n_z, first, 0)

    def more(z, carry):
        for g in range(X):

            def chunk(c, inner, g=g):
                line = (g * n_z + z) * chunks + c
                out_ref[pl.ds(line, 1), :] = line_scores(toks[g][z], line)
                return inner

            lax.fori_loop(1, chunks_of(count_ref[g * n_z + z]), chunk, 0)
        return carry

    lax.fori_loop(0, n_z, more, 0)


def combine_kernel(count_ref, place_ref, hidden_ref, values_ref, out_ref, acc, *, group):
    n_z, tok, _ = out_ref.shape
    chunks = place_ref.shape[0] // n_z
    token_of = lax.broadcasted_iota(jnp.int32, (tok, LANES), 0)

    def line_mix(line):
        here = place_ref[pl.ds(line, 1), :] == token_of
        weight = jnp.where(here, hidden_ref[pl.ds(line, 1), :], 0.0)
        high = weight.astype(jnp.bfloat16)
        low = (weight - high.astype(jnp.float32)).astype(jnp.bfloat16)
        rows = values_ref[line]
        return jnp.dot(
            jnp.concatenate([high, low], axis=1),
            jnp.concatenate([rows, rows], axis=0),
            preferred_element_type=jnp.float32,
        )

    def first(half, carry):
        zs = [half * 4 + j for j in range(4)]
        found = [line_mix(z * chunks) for z in zs]
        for z, value in zip(zs, found):
            acc[z] = value
        return carry

    lax.fori_loop(0, n_z // 4, first, 0)

    def more(z, carry):
        def chunk(c, inner):
            acc[z] += line_mix(z * chunks + c)
            return inner

        lax.fori_loop(1, chunks_of(count_ref[group * n_z + z]), chunk, 0)
        out_ref[z] = acc[z].astype(out_ref.dtype)
        return carry

    lax.fori_loop(0, n_z, more, 0)


def vmem():
    return pl.BlockSpec(memory_space=pltpu.VMEM)


def smem():
    return pl.BlockSpec(memory_space=pltpu.SMEM)


def to_each(value, axis):
    return lax.all_to_all(
        jnp.broadcast_to(value[None], (lax.axis_size(axis), *value.shape)), axis, 0, 0, tiled=True
    )


def around(shift):
    return [(i, (i + shift) % X) for i in range(X)]


def body(tokens, row_ids, row_gates, key_table, value_table, norm_gain):
    tok, width = tokens.shape
    picks = row_ids.shape[1]
    exp_dev = key_table.shape[0]
    n_ep = lax.axis_size(EP)
    cap = 3 * tok * picks // n_ep
    chunks = cap // LANES
    shift = exp_dev.bit_length() - 1
    lines = n_ep * chunks

    near = to_each(tokens, "z")
    groups = [near] + [lax.ppermute(near, "x", around(shift)) for shift in SHIFTS[1:]]
    listed = pl.pallas_call(
        lambda *refs: bucket_kernel(*refs, n_ep=n_ep, cap=cap, shift=shift),
        out_shape=jax.ShapeDtypeStruct((n_ep, 8, LANES), jnp.float32),
        in_specs=[vmem(), vmem()],
        out_specs=vmem(),
        scratch_shapes=[
            pltpu.VMEM((6 * n_ep, tok * picks), jnp.bfloat16),
            pltpu.VMEM((cap, tok * picks), jnp.bfloat16),
        ],
        interpret=INTERPRET,
        name="bucket",
    )(row_ids.T, row_gates.T)
    listed = lax.all_to_all(listed, EP, 0, 0, tiled=True)
    codes = listed[:, :chunks].astype(jnp.int32)
    gates = listed[:, chunks : 2 * chunks].reshape(lines, LANES)
    rows = (codes & (exp_dev - 1)).reshape(lines, LANES)
    place = ((codes >> shift) - 1).reshape(lines, LANES)
    count = jnp.sum((codes > 0).astype(jnp.int32), axis=(1, 2))

    n_z = n_ep // X
    picked = jax.ShapeDtypeStruct((lines, LANES, width), jnp.bfloat16)
    count, place, gates, keys, values = pl.pallas_call(
        pick_kernel,
        out_shape=(
            jax.ShapeDtypeStruct((n_ep,), jnp.int32),
            jax.ShapeDtypeStruct((lines, LANES), jnp.int32),
            jax.ShapeDtypeStruct((lines, LANES), jnp.float32),
            picked,
            picked,
        ),
        in_specs=[smem(), smem(), smem(), vmem(), vmem(), vmem(), vmem()],
        out_specs=(smem(), vmem(), vmem(), vmem(), vmem()),
        scratch_shapes=[
            pltpu.VMEM((exp_dev, width), jnp.float32),
            pltpu.VMEM((exp_dev, width), jnp.float32),
            pltpu.VMEM((LANES, width), jnp.float32),
            pltpu.VMEM((LANES, width), jnp.float32),
        ],
        interpret=INTERPRET,
        name="pick",
    )(lax.axis_index("x").reshape(1), rows, count, place, gates, key_table, value_table)
    partial_score = pl.pallas_call(
        score_kernel,
        out_shape=jax.ShapeDtypeStruct((lines, LANES), jnp.float32),
        in_specs=[smem()] + [vmem()] * 6,
        out_specs=vmem(),
        interpret=INTERPRET,
        name="score",
    )(count, place, keys, *groups)
    score = jnp.sum(lax.all_gather(partial_score, TP), axis=0)
    hidden = jnp.where(place >= 0, jax.nn.gelu(score, approximate=False) * gates, 0.0)

    def combine(group):
        per = n_z * chunks
        return pl.pallas_call(
            lambda *refs: combine_kernel(*refs, group=group),
            out_shape=jax.ShapeDtypeStruct((n_z, tok, width), jnp.bfloat16),
            grid=(1,),
            in_specs=[
                smem(),
                pl.BlockSpec((per, LANES), lambda i: (group, 0)),
                pl.BlockSpec((per, LANES), lambda i: (group, 0)),
                pl.BlockSpec((per, LANES, width), lambda i: (group, 0, 0)),
            ],
            out_specs=pl.BlockSpec((n_z, tok, width), lambda i: (0, 0, 0)),
            scratch_shapes=[pltpu.VMEM((n_z, tok, width), jnp.float32)],
            interpret=INTERPRET,
            name="combine",
        )(count, place, hidden, values)

    parts = [
        lax.ppermute(combine(g), "x", around(-SHIFTS[g])) if g else combine(g) for g in (1, 2, 3, 0)
    ]
    mine = sum(p.astype(jnp.float32) for p in parts).astype(jnp.bfloat16)
    back = lax.all_to_all(mine, "z", 0, 0, tiled=True)
    mixed = jnp.sum(back.astype(jnp.float32), axis=0)
    part = jnp.sum(mixed * mixed, axis=1).reshape(tok // LANES, LANES)
    squares = jnp.sum(to_each(part, TP), axis=0).reshape(tok)
    strength = squares / D
    return (mixed * lax.rsqrt(strength + 1e-06)[:, None] * norm_gain).astype(jnp.bfloat16)


def solution(mesh):
    ep, tp = mesh.devices.shape
    fine = Mesh(mesh.devices.reshape(Z, ep // Z, tp // 2, 2), ("z", "x", "y", "core"))
    in_specs = (P(EP, TP), P(EP, None), P(EP, None), P(EP, TP), P(EP, TP), P(TP))
    return jax.shard_map(body, mesh=fine, in_specs=in_specs, out_specs=P(EP, TP), check_vma=False)
```

```python
import jax
import jax.numpy as jnp
from jax import lax
from jax.experimental import pallas as pl
from jax.experimental.pallas import tpu as pltpu
from jax.sharding import Mesh
from jax.sharding import PartitionSpec as P

D = 2048
LANES = 128
INTERPRET = False
Z = 8
X = 4
SHIFTS = (0, 2, 1, 3)
EP = ("z", "x")
TP = ("y", "core")


def bucket_kernel(ids_ref, gates_ref, out_ref, a_ref, b_ref, *, n_ep, cap, shift):
    picks, tok = ids_ref.shape
    before = jnp.where(
        lax.broadcasted_iota(jnp.int32, (tok, tok), 0)
        < lax.broadcasted_iota(jnp.int32, (tok, tok), 1),
        1.0,
        0.0,
    ).astype(jnp.bfloat16)
    token_no = (lax.broadcasted_iota(jnp.int32, (1, tok), 1) + 1).astype(jnp.float32)
    owners = lax.broadcasted_iota(jnp.int32, (n_ep, tok), 0)
    slots = lax.broadcasted_iota(jnp.int32, (cap, tok), 0)
    base = jnp.zeros((n_ep, 1), jnp.float32)
    for k in range(picks):
        ids = ids_ref[k : k + 1, :]
        mine = (ids >> shift) == owners
        hot = jnp.where(mine, 1.0, 0.0)
        rank = base + jnp.dot(
            hot.astype(jnp.bfloat16), before, preferred_element_type=jnp.float32
        )
        place = jnp.sum(jnp.where(mine, rank, 0.0), axis=0, keepdims=True).astype(jnp.int32)
        base = base + jnp.sum(hot, axis=1, keepdims=True)
        b_ref[:, k * tok : (k + 1) * tok] = jnp.where(slots == place, 1.0, 0.0).astype(
            jnp.bfloat16
        )
        local = ids & ((1 << shift) - 1)
        gate = gates_ref[k : k + 1, :]
        gate_hi = gate.astype(jnp.bfloat16).astype(jnp.float32)
        gate_mid = (gate - gate_hi).astype(jnp.bfloat16).astype(jnp.float32)
        gate_lo = gate - gate_hi - gate_mid
        values = (
            token_no,
            (local >> 4).astype(jnp.float32),
            (local & 15).astype(jnp.float32),
            gate_hi,
            gate_mid,
            gate_lo,
        )
        for c, value in enumerate(values):
            a_ref[c * n_ep : (c + 1) * n_ep, k * tok : (k + 1) * tok] = jnp.where(
                mine, value, 0.0
            ).astype(jnp.bfloat16)
    res = lax.dot_general(
        a_ref[...], b_ref[...], (((1,), (1,)), ((), ())), preferred_element_type=jnp.float32
    )
    part = [res[c * n_ep : (c + 1) * n_ep] for c in range(6)]
    code = part[0] * float(1 << shift) + (part[1] * 16.0 + part[2])
    gates = part[3] + part[4] + part[5]
    chunks = cap // LANES
    out_ref[...] = jnp.zeros(out_ref.shape, jnp.float32)
    for j in range(chunks):
        out_ref[:, j, :] = code[:, j * LANES : (j + 1) * LANES]
        out_ref[:, chunks + j, :] = gates[:, j * LANES : (j + 1) * LANES]


def widen(table_ref, wide_ref):
    step = 256

    def one(i, carry):
        rows = pl.ds(pl.multiple_of(i * step, step), step)
        wide_ref[rows, :] = table_ref[rows, :].astype(jnp.float32)
        return carry

    lax.fori_loop(0, table_ref.shape[0] // step, one, 0)


def take_rows(rows_ref, line, wide_ref, picked, out_ref, to):
    for s in range(LANES):
        picked[pl.ds(s, 1), :] = wide_ref[pl.ds(rows_ref[line, s], 1), :]
    out_ref[to] = picked[...].astype(out_ref.dtype)


def chunks_of(count):
    return (count + LANES - 1) // LANES


def pick_kernel(
    x_ref,
    rows_ref,
    count_ref,
    place_ref,
    gate_ref,
    key_ref,
    value_ref,
    count_out,
    place_out,
    gate_out,
    keys_out,
    values_out,
    wide_k,
    wide_v,
    took_k,
    took_v,
):
    n_ep = count_ref.shape[0]
    n_z = n_ep // X
    chunks = place_ref.shape[0] // n_ep
    widen(key_ref, wide_k)
    widen(value_ref, wide_v)

    def block(i, carry):
        z = i // X
        shift = (x_ref[0] + X - i % X) % X
        slot = (shift // 2 + (shift % 2) * 2) * n_z + z
        count_out[slot] = count_ref[i]
        for c in range(chunks):
            place_out[pl.ds(slot * chunks + c, 1), :] = place_ref[pl.ds(i * chunks + c, 1), :]
            gate_out[pl.ds(slot * chunks + c, 1), :] = gate_ref[pl.ds(i * chunks + c, 1), :]

        def chunk(c, inner):
            take_rows(rows_ref, i * chunks + c, wide_k, took_k, keys_out, slot * chunks + c)
            take_rows(rows_ref, i * chunks + c, wide_v, took_v, values_out, slot * chunks + c)
            return inner

        lax.fori_loop(0, chunks_of(count_ref[i]), chunk, 0)
        return carry

    lax.fori_loop(0, n_ep, block, 0)


def score_kernel(count_ref, place_ref, keys_ref, tok0, tok1, tok2, tok3, out_ref, found_ref):
    toks = (tok0, tok1, tok2, tok3)
    n_z, tok, _ = tok0.shape
    chunks = place_ref.shape[0] // (X * n_z)
    found_ref[...] = jnp.zeros(found_ref.shape, jnp.float32)
    token_of = lax.broadcasted_iota(jnp.int32, (tok, LANES), 0)

    def line_scores(tokens, line):
        prod = lax.dot_general(
            tokens, keys_ref[line], (((1,), (1,)), ((), ())), preferred_element_type=jnp.float32
        )
        here = place_ref[pl.ds(line, 1), :] == token_of
        return jnp.sum(jnp.where(here, prod, 0.0), axis=0, keepdims=True)

    def first(z, carry):
        lines = [(g * n_z + z) * chunks for g in range(X)]
        found = [line_scores(toks[g][z], lines[g]) for g in range(X)]
        for line, value in zip(lines, found):
            found_ref[pl.ds(line, 1), :] = value
        return carry

    lax.fori_loop(0, n_z, first, 0)

    def more(z, carry):
        for g in range(X):

            def chunk(c, inner, g=g):
                line = (g * n_z + z) * chunks + c
                found_ref[pl.ds(line, 1), :] = line_scores(toks[g][z], line)
                return inner

            lax.fori_loop(1, chunks_of(count_ref[g * n_z + z]), chunk, 0)
        return carry

    lax.fori_loop(0, n_z, more, 0)
    out_ref[...] = found_ref[...].astype(out_ref.dtype)


def combine_kernel(count_ref, place_ref, hidden_ref, values_ref, out_ref, acc, *, group):
    n_z, tok, _ = out_ref.shape
    chunks = place_ref.shape[0] // n_z
    token_of = lax.broadcasted_iota(jnp.int32, (tok, LANES), 0)

    def line_mix(line):
        here = place_ref[pl.ds(line, 1), :] == token_of
        weight = jnp.where(here, hidden_ref[pl.ds(line, 1), :], 0.0)
        high = weight.astype(jnp.bfloat16)
        low = (weight - high.astype(jnp.float32)).astype(jnp.bfloat16)
        rows = values_ref[line]
        return jnp.dot(
            jnp.concatenate([high, low], axis=1),
            jnp.concatenate([rows, rows], axis=0),
            preferred_element_type=jnp.float32,
        )

    def first(half, carry):
        zs = [half * 4 + j for j in range(4)]
        found = [line_mix(z * chunks) for z in zs]
        for z, value in zip(zs, found):
            acc[z] = value
        return carry

    lax.fori_loop(0, n_z // 4, first, 0)

    def more(z, carry):
        def chunk(c, inner):
            acc[z] += line_mix(z * chunks + c)
            return inner

        lax.fori_loop(1, chunks_of(count_ref[group * n_z + z]), chunk, 0)
        out_ref[z] = acc[z].astype(out_ref.dtype)
        return carry

    lax.fori_loop(0, n_z, more, 0)


def vmem():
    return pl.BlockSpec(memory_space=pltpu.VMEM)


def smem():
    return pl.BlockSpec(memory_space=pltpu.SMEM)


def to_each(value, axis):
    return lax.all_to_all(
        jnp.broadcast_to(value[None], (lax.axis_size(axis), *value.shape)), axis, 0, 0, tiled=True
    )


def around(shift):
    return [(i, (i + shift) % X) for i in range(X)]


def body(tokens, row_ids, row_gates, key_table, value_table, norm_gain):
    tok, width = tokens.shape
    picks = row_ids.shape[1]
    exp_dev = key_table.shape[0]
    n_ep = lax.axis_size(EP)
    cap = 3 * tok * picks // n_ep
    chunks = cap // LANES
    shift = exp_dev.bit_length() - 1
    lines = n_ep * chunks

    near = lax.all_gather(tokens, "z")
    groups = [near] + [lax.ppermute(near, "x", around(shift)) for shift in SHIFTS[1:]]
    listed = pl.pallas_call(
        lambda *refs: bucket_kernel(*refs, n_ep=n_ep, cap=cap, shift=shift),
        out_shape=jax.ShapeDtypeStruct((n_ep, 8, LANES), jnp.float32),
        in_specs=[vmem(), vmem()],
        out_specs=vmem(),
        scratch_shapes=[
            pltpu.VMEM((6 * n_ep, tok * picks), jnp.bfloat16),
            pltpu.VMEM((cap, tok * picks), jnp.bfloat16),
        ],
        interpret=INTERPRET,
        name="bucket",
    )(row_ids.T, row_gates.T)
    listed = lax.all_to_all(listed, EP, 0, 0, tiled=True)
    codes = listed[:, :chunks].astype(jnp.int32)
    gates = listed[:, chunks : 2 * chunks].reshape(lines, LANES)
    rows = (codes & (exp_dev - 1)).reshape(lines, LANES)
    place = ((codes >> shift) - 1).reshape(lines, LANES)
    count = jnp.sum((codes > 0).astype(jnp.int32), axis=(1, 2))

    n_z = n_ep // X
    picked = jax.ShapeDtypeStruct((lines, LANES, width), jnp.bfloat16)
    count, place, gates, keys, values = pl.pallas_call(
        pick_kernel,
        out_shape=(
            jax.ShapeDtypeStruct((n_ep,), jnp.int32),
            jax.ShapeDtypeStruct((lines, LANES), jnp.int32),
            jax.ShapeDtypeStruct((lines, LANES), jnp.float32),
            picked,
            picked,
        ),
        in_specs=[smem(), smem(), smem(), vmem(), vmem(), vmem(), vmem()],
        out_specs=(smem(), vmem(), vmem(), vmem(), vmem()),
        scratch_shapes=[
            pltpu.VMEM((exp_dev, width), jnp.float32),
            pltpu.VMEM((exp_dev, width), jnp.float32),
            pltpu.VMEM((LANES, width), jnp.float32),
            pltpu.VMEM((LANES, width), jnp.float32),
        ],
        interpret=INTERPRET,
        name="pick",
    )(lax.axis_index("x").reshape(1), rows, count, place, gates, key_table, value_table)
    partial_score = pl.pallas_call(
        score_kernel,
        out_shape=jax.ShapeDtypeStruct((lines, LANES), jnp.bfloat16),
        in_specs=[smem()] + [vmem()] * 6,
        out_specs=vmem(),
        scratch_shapes=[pltpu.VMEM((lines, LANES), jnp.float32)],
        interpret=INTERPRET,
        name="score",
    )(count, place, keys, *groups)
    score = jnp.sum(lax.all_gather(partial_score, TP).astype(jnp.float32), axis=0)
    hidden = jnp.where(place >= 0, jax.nn.gelu(score, approximate=False) * gates, 0.0)

    def combine(group):
        per = n_z * chunks
        return pl.pallas_call(
            lambda *refs: combine_kernel(*refs, group=group),
            out_shape=jax.ShapeDtypeStruct((n_z, tok, width), jnp.bfloat16),
            grid=(1,),
            in_specs=[
                smem(),
                pl.BlockSpec((per, LANES), lambda i: (group, 0)),
                pl.BlockSpec((per, LANES), lambda i: (group, 0)),
                pl.BlockSpec((per, LANES, width), lambda i: (group, 0, 0)),
            ],
            out_specs=pl.BlockSpec((n_z, tok, width), lambda i: (0, 0, 0)),
            scratch_shapes=[pltpu.VMEM((n_z, tok, width), jnp.float32)],
            interpret=INTERPRET,
            name="combine",
        )(count, place, hidden, values)

    parts = []
    for g in (1, 2, 3, 0):
        part = combine(g)
        if g:
            part = lax.ppermute(part, "x", around(-SHIFTS[g]))
        parts.append(part)
    mine = sum(p.astype(jnp.float32) for p in parts).astype(jnp.bfloat16)
    back = lax.all_to_all(mine, "z", 0, 0, tiled=True)
    mixed = jnp.sum(back.astype(jnp.float32), axis=0)
    part = jnp.sum(mixed * mixed, axis=1).reshape(tok // LANES, LANES)
    squares = jnp.sum(to_each(part, TP), axis=0).reshape(tok)
    strength = squares / D
    return (mixed * lax.rsqrt(strength + 1e-06)[:, None] * norm_gain).astype(jnp.bfloat16)


def solution(mesh):
    ep, tp = mesh.devices.shape
    fine = Mesh(mesh.devices.reshape(Z, ep // Z, tp // 2, 2), ("z", "x", "y", "core"))
    in_specs = (P(EP, TP), P(EP, None), P(EP, None), P(EP, TP), P(EP, TP), P(TP))

    return jax.shard_map(body, mesh=fine, in_specs=in_specs, out_specs=P(EP, TP), check_vma=False)
```

```python
import jax
import jax.numpy as jnp
from jax import lax
from jax.experimental import pallas as pl
from jax.experimental.pallas import tpu as pltpu
from jax.sharding import Mesh
from jax.sharding import PartitionSpec as P

D = 2048
LANES = 128
INTERPRET = False
Z = 8
X = 4
ROOM = 24 * 1024 * 1024
SHIFTS = (0, 2, 1, 3)
EP = ("z", "x")
TP = ("y", "core")


def bucket_kernel(ids_ref, gates_ref, out_ref, a_ref, b_ref, *, n_ep, cap, shift):
    picks, tok = ids_ref.shape
    before = jnp.where(
        lax.broadcasted_iota(jnp.int32, (tok, tok), 0)
        < lax.broadcasted_iota(jnp.int32, (tok, tok), 1),
        1.0,
        0.0,
    ).astype(jnp.bfloat16)
    token_no = (lax.broadcasted_iota(jnp.int32, (1, tok), 1) + 1).astype(jnp.float32)
    owners = lax.broadcasted_iota(jnp.int32, (n_ep, tok), 0)
    slots = lax.broadcasted_iota(jnp.int32, (cap, tok), 0)
    base = jnp.zeros((n_ep, 1), jnp.float32)
    for k in range(picks):
        ids = ids_ref[k : k + 1, :]
        mine = (ids >> shift) == owners
        hot = jnp.where(mine, 1.0, 0.0)
        rank = base + jnp.dot(
            hot.astype(jnp.bfloat16), before, preferred_element_type=jnp.float32
        )
        place = jnp.sum(jnp.where(mine, rank, 0.0), axis=0, keepdims=True).astype(jnp.int32)
        base = base + jnp.sum(hot, axis=1, keepdims=True)
        b_ref[:, k * tok : (k + 1) * tok] = jnp.where(slots == place, 1.0, 0.0).astype(
            jnp.bfloat16
        )
        local = ids & ((1 << shift) - 1)
        gate = gates_ref[k : k + 1, :]
        gate_hi = gate.astype(jnp.bfloat16).astype(jnp.float32)
        gate_mid = (gate - gate_hi).astype(jnp.bfloat16).astype(jnp.float32)
        gate_lo = gate - gate_hi - gate_mid
        values = (
            token_no,
            (local >> 4).astype(jnp.float32),
            (local & 15).astype(jnp.float32),
            gate_hi,
            gate_mid,
            gate_lo,
        )
        for c, value in enumerate(values):
            a_ref[c * n_ep : (c + 1) * n_ep, k * tok : (k + 1) * tok] = jnp.where(
                mine, value, 0.0
            ).astype(jnp.bfloat16)
    res = lax.dot_general(
        a_ref[...], b_ref[...], (((1,), (1,)), ((), ())), preferred_element_type=jnp.float32
    )
    part = [res[c * n_ep : (c + 1) * n_ep] for c in range(6)]
    code = part[0] * float(1 << shift) + (part[1] * 16.0 + part[2])
    gates = part[3] + part[4] + part[5]
    chunks = cap // LANES
    out_ref[...] = jnp.zeros(out_ref.shape, jnp.float32)
    for j in range(chunks):
        out_ref[:, j, :] = code[:, j * LANES : (j + 1) * LANES]
        out_ref[:, chunks + j, :] = gates[:, j * LANES : (j + 1) * LANES]


def widen(table_ref, wide_ref):
    step = 256

    def one(i, carry):
        rows = pl.ds(pl.multiple_of(i * step, step), step)
        wide_ref[rows, :] = table_ref[rows, :].astype(jnp.float32)
        return carry

    lax.fori_loop(0, table_ref.shape[0] // step, one, 0)


def take_rows(rows_ref, line, wide_ref, picked, out_ref, to):
    for s in range(LANES):
        picked[pl.ds(s, 1), :] = wide_ref[pl.ds(rows_ref[line, s], 1), :]
    out_ref[to] = picked[...].astype(out_ref.dtype)


def chunks_of(count):
    return (count + LANES - 1) // LANES


def pick_kernel(
    x_ref,
    rows_ref,
    count_ref,
    place_ref,
    gate_ref,
    key_ref,
    value_ref,
    count_out,
    place_out,
    gate_out,
    keys_out,
    values_out,
    wide_k,
    wide_v,
    took_k,
    took_v,
):
    n_ep = count_ref.shape[0]
    n_z = n_ep // X
    chunks = place_ref.shape[0] // n_ep
    widen(key_ref, wide_k)
    widen(value_ref, wide_v)

    def block(i, carry):
        z = i // X
        shift = (x_ref[0] + X - i % X) % X
        slot = (shift // 2 + (shift % 2) * 2) * n_z + z
        count_out[slot] = count_ref[i]
        for c in range(chunks):
            place_out[pl.ds(slot * chunks + c, 1), :] = place_ref[pl.ds(i * chunks + c, 1), :]
            gate_out[pl.ds(slot * chunks + c, 1), :] = gate_ref[pl.ds(i * chunks + c, 1), :]

        def chunk(c, inner):
            take_rows(rows_ref, i * chunks + c, wide_k, took_k, keys_out, slot * chunks + c)
            take_rows(rows_ref, i * chunks + c, wide_v, took_v, values_out, slot * chunks + c)
            return inner

        lax.fori_loop(0, chunks_of(count_ref[i]), chunk, 0)
        return carry

    lax.fori_loop(0, n_ep, block, 0)


def score_kernel(count_ref, place_ref, keys_ref, tok0, tok1, tok2, tok3, out_ref):
    toks = (tok0, tok1, tok2, tok3)
    n_z, tok, _ = tok0.shape
    chunks = place_ref.shape[0] // (X * n_z)
    out_ref[...] = jnp.zeros(out_ref.shape, jnp.float32)
    token_of = lax.broadcasted_iota(jnp.int32, (tok, LANES), 0)

    def line_scores(tokens, line):
        prod = lax.dot_general(
            tokens, keys_ref[line], (((1,), (1,)), ((), ())), preferred_element_type=jnp.float32
        )
        here = place_ref[pl.ds(line, 1), :] == token_of
        return jnp.sum(jnp.where(here, prod, 0.0), axis=0, keepdims=True)

    def first(z, carry):
        lines = [(g * n_z + z) * chunks for g in range(X)]
        found = [line_scores(toks[g][z], lines[g]) for g in range(X)]
        for line, value in zip(lines, found):
            out_ref[pl.ds(line, 1), :] = value
        return carry

    lax.fori_loop(0, n_z, first, 0)

    def more(z, carry):
        for g in range(X):

            def chunk(c, inner, g=g):
                line = (g * n_z + z) * chunks + c
                out_ref[pl.ds(line, 1), :] = line_scores(toks[g][z], line)
                return inner

            lax.fori_loop(1, chunks_of(count_ref[g * n_z + z]), chunk, 0)
        return carry

    lax.fori_loop(0, n_z, more, 0)


def combine_kernel(count_ref, place_ref, hidden_ref, values_ref, out_ref, acc, *, group):
    n_z, tok, _ = out_ref.shape
    chunks = place_ref.shape[0] // (X * n_z)
    token_of = lax.broadcasted_iota(jnp.int32, (tok, LANES), 0)

    def line_mix(z, c):
        line = (group * n_z + z) * chunks + c
        here = place_ref[pl.ds(line, 1), :] == token_of
        weight = jnp.where(here, hidden_ref[pl.ds(line, 1), :], 0.0)
        high = weight.astype(jnp.bfloat16)
        low = (weight - high.astype(jnp.float32)).astype(jnp.bfloat16)
        rows = values_ref[line]
        return jnp.dot(
            jnp.concatenate([high, low], axis=1),
            jnp.concatenate([rows, rows], axis=0),
            preferred_element_type=jnp.float32,
        )

    def first(half, carry):
        zs = [half * 4 + j for j in range(4)]
        found = [line_mix(z, 0) for z in zs]
        for z, value in zip(zs, found):
            acc[z] = value
        return carry

    lax.fori_loop(0, n_z // 4, first, 0)

    def more(z, carry):
        def chunk(c, inner):
            acc[z] += line_mix(z, c)
            return inner

        lax.fori_loop(1, chunks_of(count_ref[group * n_z + z]), chunk, 0)
        out_ref[z] = acc[z].astype(out_ref.dtype)
        return carry

    lax.fori_loop(0, n_z, more, 0)


def vmem():
    return pl.BlockSpec(memory_space=pltpu.VMEM)


def made(shape, dtype):
    return jax.ShapeDtypeStruct(shape, dtype) if INTERPRET else pltpu.VMEM(shape, dtype)


def held(value):
    return value if INTERPRET else pltpu.with_memory_space_constraint(value, pltpu.VMEM)


def smem():
    return pl.BlockSpec(memory_space=pltpu.SMEM)


def to_each(value, axis):
    return lax.all_to_all(
        jnp.broadcast_to(value[None], (lax.axis_size(axis), *value.shape)), axis, 0, 0, tiled=True
    )


def around(shift):
    return [(i, (i + shift) % X) for i in range(X)]


def body(tokens, row_ids, row_gates, key_table, value_table, norm_gain):
    tok, width = tokens.shape
    picks = row_ids.shape[1]
    exp_dev = key_table.shape[0]
    n_ep = lax.axis_size(EP)
    cap = 3 * tok * picks // n_ep
    chunks = cap // LANES
    shift = exp_dev.bit_length() - 1
    lines = n_ep * chunks

    near = lax.all_gather(tokens, "z")
    groups = [near] + [lax.ppermute(near, "x", around(shift)) for shift in SHIFTS[1:]]
    listed = pl.pallas_call(
        lambda *refs: bucket_kernel(*refs, n_ep=n_ep, cap=cap, shift=shift),
        out_shape=jax.ShapeDtypeStruct((n_ep, 8, LANES), jnp.float32),
        in_specs=[vmem(), vmem()],
        out_specs=vmem(),
        scratch_shapes=[
            pltpu.VMEM((6 * n_ep, tok * picks), jnp.bfloat16),
            pltpu.VMEM((cap, tok * picks), jnp.bfloat16),
        ],
        interpret=INTERPRET,
        compiler_params=pltpu.CompilerParams(vmem_limit_bytes=ROOM),
        name="bucket",
    )(row_ids.T, row_gates.T)
    listed = lax.all_to_all(listed, EP, 0, 0, tiled=True)
    codes = listed[:, :chunks].astype(jnp.int32)
    gates = listed[:, chunks : 2 * chunks].reshape(lines, LANES)
    rows = (codes & (exp_dev - 1)).reshape(lines, LANES)
    place = ((codes >> shift) - 1).reshape(lines, LANES)
    count = jnp.sum((codes > 0).astype(jnp.int32), axis=(1, 2))

    n_z = n_ep // X
    picked = made((lines, LANES, width), jnp.bfloat16)
    count, place, gates, keys, values = pl.pallas_call(
        pick_kernel,
        out_shape=(
            jax.ShapeDtypeStruct((n_ep,), jnp.int32),
            jax.ShapeDtypeStruct((lines, LANES), jnp.int32),
            jax.ShapeDtypeStruct((lines, LANES), jnp.float32),
            picked,
            picked,
        ),
        in_specs=[smem(), smem(), smem(), vmem(), vmem(), vmem(), vmem()],
        out_specs=(smem(), vmem(), vmem(), vmem(), vmem()),
        scratch_shapes=[
            pltpu.VMEM((exp_dev, width), jnp.float32),
            pltpu.VMEM((exp_dev, width), jnp.float32),
            pltpu.VMEM((LANES, width), jnp.float32),
            pltpu.VMEM((LANES, width), jnp.float32),
        ],
        interpret=INTERPRET,
        compiler_params=pltpu.CompilerParams(vmem_limit_bytes=ROOM),
        name="pick",
    )(lax.axis_index("x").reshape(1), rows, count, place, gates, key_table, value_table)
    partial_score = pl.pallas_call(
        score_kernel,
        out_shape=jax.ShapeDtypeStruct((lines, LANES), jnp.float32),
        in_specs=[smem()] + [vmem()] * 6,
        out_specs=vmem(),
        interpret=INTERPRET,
        compiler_params=pltpu.CompilerParams(vmem_limit_bytes=ROOM),
        name="score",
    )(count, place, held(keys), *[held(g) for g in groups])
    score = jnp.sum(lax.all_gather(partial_score, TP), axis=0)
    hidden = jnp.where(place >= 0, jax.nn.gelu(score, approximate=False) * gates, 0.0)

    def combine(group):
        return pl.pallas_call(
            lambda *refs: combine_kernel(*refs, group=group),
            out_shape=made((n_z, tok, width), jnp.bfloat16),
            in_specs=[smem(), vmem(), vmem(), vmem()],
            out_specs=vmem(),
            scratch_shapes=[pltpu.VMEM((n_z, tok, width), jnp.float32)],
            interpret=INTERPRET,
            compiler_params=pltpu.CompilerParams(vmem_limit_bytes=ROOM),
            name="combine",
        )(count, held(place), held(hidden), held(values))

    parts = []
    for g in (1, 2, 3, 0):
        part = combine(g)
        if g:
            part = lax.ppermute(part, "x", around(-SHIFTS[g]))
        parts.append(part)
    mine = sum(p.astype(jnp.float32) for p in parts).astype(jnp.bfloat16)
    back = lax.all_to_all(mine, "z", 0, 0, tiled=True)
    mixed = jnp.sum(back.astype(jnp.float32), axis=0)
    part = jnp.sum(mixed * mixed, axis=1).reshape(tok // LANES, LANES)
    squares = jnp.sum(to_each(part, TP), axis=0).reshape(tok)
    strength = squares / D
    return (mixed * lax.rsqrt(strength + 1e-06)[:, None] * norm_gain).astype(jnp.bfloat16)


def solution(mesh):
    ep, tp = mesh.devices.shape
    fine = Mesh(mesh.devices.reshape(Z, ep // Z, tp // 2, 2), ("z", "x", "y", "core"))
    in_specs = (P(EP, TP), P(EP, None), P(EP, None), P(EP, TP), P(EP, TP), P(TP))

    return jax.shard_map(body, mesh=fine, in_specs=in_specs, out_specs=P(EP, TP), check_vma=False)
```

```python
import jax
import jax.numpy as jnp
from jax import lax
from jax.experimental import pallas as pl
from jax.experimental.pallas import tpu as pltpu
from jax.sharding import Mesh
from jax.sharding import PartitionSpec as P

D = 2048
LANES = 128
INTERPRET = False
Z = 8
X = 4
ROOM = 24 * 1024 * 1024
SHIFTS = (0, 2, 1, 3)
EP = ("z", "x")
TP = ("y", "core")


def bucket_kernel(ids_ref, gates_ref, out_ref, a_ref, b_ref, *, n_ep, cap, shift):
    picks, tok = ids_ref.shape
    before = jnp.where(
        lax.broadcasted_iota(jnp.int32, (tok, tok), 0)
        < lax.broadcasted_iota(jnp.int32, (tok, tok), 1),
        1.0,
        0.0,
    ).astype(jnp.bfloat16)
    token_no = (lax.broadcasted_iota(jnp.int32, (1, tok), 1) + 1).astype(jnp.float32)
    owners = lax.broadcasted_iota(jnp.int32, (n_ep, tok), 0)
    slots = lax.broadcasted_iota(jnp.int32, (cap, tok), 0)
    base = jnp.zeros((n_ep, 1), jnp.float32)
    for k in range(picks):
        ids = ids_ref[k : k + 1, :]
        mine = (ids >> shift) == owners
        hot = jnp.where(mine, 1.0, 0.0)
        rank = base + jnp.dot(
            hot.astype(jnp.bfloat16), before, preferred_element_type=jnp.float32
        )
        place = jnp.sum(jnp.where(mine, rank, 0.0), axis=0, keepdims=True).astype(jnp.int32)
        base = base + jnp.sum(hot, axis=1, keepdims=True)
        b_ref[:, k * tok : (k + 1) * tok] = jnp.where(slots == place, 1.0, 0.0).astype(
            jnp.bfloat16
        )
        local = ids & ((1 << shift) - 1)
        gate = gates_ref[k : k + 1, :]
        gate_hi = gate.astype(jnp.bfloat16).astype(jnp.float32)
        gate_mid = (gate - gate_hi).astype(jnp.bfloat16).astype(jnp.float32)
        gate_lo = gate - gate_hi - gate_mid
        values = (
            token_no,
            (local >> 4).astype(jnp.float32),
            (local & 15).astype(jnp.float32),
            gate_hi,
            gate_mid,
            gate_lo,
        )
        for c, value in enumerate(values):
            a_ref[c * n_ep : (c + 1) * n_ep, k * tok : (k + 1) * tok] = jnp.where(
                mine, value, 0.0
            ).astype(jnp.bfloat16)
    res = lax.dot_general(
        a_ref[...], b_ref[...], (((1,), (1,)), ((), ())), preferred_element_type=jnp.float32
    )
    part = [res[c * n_ep : (c + 1) * n_ep] for c in range(6)]
    code = part[0] * float(1 << shift) + (part[1] * 16.0 + part[2])
    gates = part[3] + part[4] + part[5]
    chunks = cap // LANES
    out_ref[...] = jnp.zeros(out_ref.shape, jnp.float32)
    for j in range(chunks):
        out_ref[:, j, :] = code[:, j * LANES : (j + 1) * LANES]
        out_ref[:, chunks + j, :] = gates[:, j * LANES : (j + 1) * LANES]


def widen(table_ref, wide_ref):
    step = 256

    def one(i, carry):
        rows = pl.ds(pl.multiple_of(i * step, step), step)
        wide_ref[rows, :] = table_ref[rows, :].astype(jnp.float32)
        return carry

    lax.fori_loop(0, table_ref.shape[0] // step, one, 0)


def take_rows(rows_ref, line, wide_ref, picked, out_ref, to):
    for s in range(LANES):
        picked[pl.ds(s, 1), :] = wide_ref[pl.ds(rows_ref[line, s], 1), :]
    out_ref[to] = picked[...].astype(out_ref.dtype)


def chunks_of(count):
    return (count + LANES - 1) // LANES


def pick_kernel(
    x_ref,
    rows_ref,
    count_ref,
    place_ref,
    gate_ref,
    key_ref,
    value_ref,
    count_out,
    place_out,
    gate_out,
    keys_out,
    values_out,
    wide_k,
    wide_v,
    took_k,
    took_v,
):
    n_ep = count_ref.shape[0]
    n_z = n_ep // X
    chunks = place_ref.shape[0] // n_ep
    widen(key_ref, wide_k)
    widen(value_ref, wide_v)

    def block(i, carry):
        z = i // X
        shift = (x_ref[0] + X - i % X) % X
        slot = (shift // 2 + (shift % 2) * 2) * n_z + z
        count_out[slot] = count_ref[i]
        for c in range(chunks):
            place_out[pl.ds(slot * chunks + c, 1), :] = place_ref[pl.ds(i * chunks + c, 1), :]
            gate_out[pl.ds(slot * chunks + c, 1), :] = gate_ref[pl.ds(i * chunks + c, 1), :]

        def chunk(c, inner):
            take_rows(rows_ref, i * chunks + c, wide_k, took_k, keys_out, slot * chunks + c)
            take_rows(rows_ref, i * chunks + c, wide_v, took_v, values_out, slot * chunks + c)
            return inner

        lax.fori_loop(0, chunks_of(count_ref[i]), chunk, 0)
        return carry

    lax.fori_loop(0, n_ep, block, 0)


def score_kernel(count_ref, place_ref, keys_ref, tok0, tok1, tok2, tok3, out_ref):
    toks = (tok0, tok1, tok2, tok3)
    n_z, tok, _ = tok0.shape
    chunks = place_ref.shape[0] // (X * n_z)
    out_ref[...] = jnp.zeros(out_ref.shape, jnp.float32)
    token_of = lax.broadcasted_iota(jnp.int32, (tok, LANES), 0)

    def line_scores(tokens, line):
        prod = lax.dot_general(
            tokens, keys_ref[line], (((1,), (1,)), ((), ())), preferred_element_type=jnp.float32
        )
        here = place_ref[pl.ds(line, 1), :] == token_of
        return jnp.sum(jnp.where(here, prod, 0.0), axis=0, keepdims=True)

    def first(z, carry):
        lines = [(g * n_z + z) * chunks for g in range(X)]
        found = [line_scores(toks[g][z], lines[g]) for g in range(X)]
        for line, value in zip(lines, found):
            out_ref[pl.ds(line, 1), :] = value
        return carry

    lax.fori_loop(0, n_z, first, 0)

    def more(z, carry):
        for g in range(X):

            def chunk(c, inner, g=g):
                line = (g * n_z + z) * chunks + c
                out_ref[pl.ds(line, 1), :] = line_scores(toks[g][z], line)
                return inner

            lax.fori_loop(1, chunks_of(count_ref[g * n_z + z]), chunk, 0)
        return carry

    lax.fori_loop(0, n_z, more, 0)


def combine_kernel(count_ref, place_ref, hidden_ref, values_ref, out_ref, acc, *, group):
    n_z, tok, _ = out_ref.shape
    chunks = place_ref.shape[0] // (X * n_z)
    token_of = lax.broadcasted_iota(jnp.int32, (tok, LANES), 0)

    def line_mix(z, c):
        line = (group * n_z + z) * chunks + c
        here = place_ref[pl.ds(line, 1), :] == token_of
        weight = jnp.where(here, hidden_ref[pl.ds(line, 1), :], 0.0)
        high = weight.astype(jnp.bfloat16)
        low = (weight - high.astype(jnp.float32)).astype(jnp.bfloat16)
        rows = values_ref[line]
        return jnp.dot(
            jnp.concatenate([high, low], axis=1),
            jnp.concatenate([rows, rows], axis=0),
            preferred_element_type=jnp.float32,
        )

    def first(half, carry):
        zs = [half * 4 + j for j in range(4)]
        found = [line_mix(z, 0) for z in zs]
        for z, value in zip(zs, found):
            acc[z] = value
        return carry

    lax.fori_loop(0, n_z // 4, first, 0)

    def more(z, carry):
        def chunk(c, inner):
            acc[z] += line_mix(z, c)
            return inner

        lax.fori_loop(1, chunks_of(count_ref[group * n_z + z]), chunk, 0)
        out_ref[z] = acc[z].astype(out_ref.dtype)
        return carry

    lax.fori_loop(0, n_z, more, 0)


def vmem():
    return pl.BlockSpec(memory_space=pltpu.VMEM)


def made(shape, dtype):
    return jax.ShapeDtypeStruct(shape, dtype) if INTERPRET else pltpu.VMEM(shape, dtype)


def held(value, where=pltpu.VMEM):
    return value if INTERPRET else pltpu.with_memory_space_constraint(value, where)


def smem():
    return pl.BlockSpec(memory_space=pltpu.SMEM)


def to_each(value, axis):
    return lax.all_to_all(
        jnp.broadcast_to(value[None], (lax.axis_size(axis), *value.shape)), axis, 0, 0, tiled=True
    )


def around(shift):
    return [(i, (i + shift) % X) for i in range(X)]


def body(tokens, row_ids, row_gates, key_table, value_table, norm_gain):
    tok, width = tokens.shape
    picks = row_ids.shape[1]
    exp_dev = key_table.shape[0]
    n_ep = lax.axis_size(EP)
    cap = 3 * tok * picks // n_ep
    chunks = cap // LANES
    shift = exp_dev.bit_length() - 1
    lines = n_ep * chunks

    near = to_each(tokens, "z")
    groups = [near] + [lax.ppermute(near, "x", around(shift)) for shift in SHIFTS[1:]]
    listed = pl.pallas_call(
        lambda *refs: bucket_kernel(*refs, n_ep=n_ep, cap=cap, shift=shift),
        out_shape=jax.ShapeDtypeStruct((n_ep, 8, LANES), jnp.float32),
        in_specs=[vmem(), vmem()],
        out_specs=vmem(),
        scratch_shapes=[
            pltpu.VMEM((6 * n_ep, tok * picks), jnp.bfloat16),
            pltpu.VMEM((cap, tok * picks), jnp.bfloat16),
        ],
        interpret=INTERPRET,
        compiler_params=pltpu.CompilerParams(vmem_limit_bytes=ROOM),
        name="bucket",
    )(row_ids.T, row_gates.T)
    listed = lax.all_to_all(listed, EP, 0, 0, tiled=True)
    codes = listed[:, :chunks].astype(jnp.int32)
    gates = listed[:, chunks : 2 * chunks].reshape(lines, LANES)
    rows = (codes & (exp_dev - 1)).reshape(lines, LANES)
    place = ((codes >> shift) - 1).reshape(lines, LANES)
    count = jnp.sum((codes > 0).astype(jnp.int32), axis=(1, 2))

    n_z = n_ep // X
    picked = made((lines, LANES, width), jnp.bfloat16)
    count, place, gates, keys, values = pl.pallas_call(
        pick_kernel,
        out_shape=(
            jax.ShapeDtypeStruct((n_ep,), jnp.int32),
            jax.ShapeDtypeStruct((lines, LANES), jnp.int32),
            jax.ShapeDtypeStruct((lines, LANES), jnp.float32),
            picked,
            picked,
        ),
        in_specs=[smem(), smem(), smem(), vmem(), vmem(), vmem(), vmem()],
        out_specs=(smem(), vmem(), vmem(), vmem(), vmem()),
        scratch_shapes=[
            pltpu.VMEM((exp_dev, width), jnp.float32),
            pltpu.VMEM((exp_dev, width), jnp.float32),
            pltpu.VMEM((LANES, width), jnp.float32),
            pltpu.VMEM((LANES, width), jnp.float32),
        ],
        interpret=INTERPRET,
        compiler_params=pltpu.CompilerParams(vmem_limit_bytes=ROOM),
        name="pick",
    )(
        lax.axis_index("x").reshape(1),
        rows,
        count,
        place,
        gates,
        held(key_table, pltpu.HBM),
        held(value_table, pltpu.HBM),
    )
    partial_score = pl.pallas_call(
        score_kernel,
        out_shape=jax.ShapeDtypeStruct((lines, LANES), jnp.float32),
        in_specs=[smem()] + [vmem()] * 6,
        out_specs=vmem(),
        interpret=INTERPRET,
        compiler_params=pltpu.CompilerParams(vmem_limit_bytes=ROOM),
        name="score",
    )(count, place, held(keys), *[held(g) for g in groups])
    score = jnp.sum(lax.all_gather(partial_score, TP), axis=0)
    hidden = jnp.where(place >= 0, jax.nn.gelu(score, approximate=False) * gates, 0.0)

    def combine(group):
        return pl.pallas_call(
            lambda *refs: combine_kernel(*refs, group=group),
            out_shape=made((n_z, tok, width), jnp.bfloat16),
            in_specs=[smem(), vmem(), vmem(), vmem()],
            out_specs=vmem(),
            scratch_shapes=[pltpu.VMEM((n_z, tok, width), jnp.float32)],
            interpret=INTERPRET,
            compiler_params=pltpu.CompilerParams(vmem_limit_bytes=ROOM),
            name="combine",
        )(count, held(place), held(hidden), held(values))

    parts = []
    for g in (1, 2, 3, 0):
        part = combine(g)
        if g:
            part = lax.ppermute(part, "x", around(-SHIFTS[g]))
        parts.append(part)
    mine = sum(p.astype(jnp.float32) for p in parts).astype(jnp.bfloat16)
    back = lax.all_to_all(mine, "z", 0, 0, tiled=True)
    mixed = jnp.sum(back.astype(jnp.float32), axis=0)
    part = jnp.sum(mixed * mixed, axis=1).reshape(tok // LANES, LANES)
    squares = jnp.sum(to_each(part, TP), axis=0).reshape(tok)
    strength = squares / D
    return (mixed * lax.rsqrt(strength + 1e-06)[:, None] * norm_gain).astype(jnp.bfloat16)


def solution(mesh):
    ep, tp = mesh.devices.shape
    fine = Mesh(mesh.devices.reshape(Z, ep // Z, tp // 2, 2), ("z", "x", "y", "core"))
    in_specs = (P(EP, TP), P(EP, None), P(EP, None), P(EP, TP), P(EP, TP), P(TP))

    return jax.shard_map(body, mesh=fine, in_specs=in_specs, out_specs=P(EP, TP), check_vma=False)
```

```python
import jax
import jax.numpy as jnp
from jax import lax
from jax.experimental import pallas as pl
from jax.experimental.pallas import tpu as pltpu
from jax.sharding import Mesh
from jax.sharding import PartitionSpec as P

D = 2048
LANES = 128
INTERPRET = False
Z = 8
X = 4
ROOM = 24 * 1024 * 1024
SHIFTS = (0, 2, 1, 3)
EP = ("z", "x")
TP = ("y", "core")


def bucket_kernel(ids_ref, gates_ref, out_ref, a_ref, b_ref, *, n_ep, cap, shift):
    picks, tok = ids_ref.shape
    before = jnp.where(
        lax.broadcasted_iota(jnp.int32, (tok, tok), 0)
        < lax.broadcasted_iota(jnp.int32, (tok, tok), 1),
        1.0,
        0.0,
    ).astype(jnp.bfloat16)
    token_no = (lax.broadcasted_iota(jnp.int32, (1, tok), 1) + 1).astype(jnp.float32)
    owners = lax.broadcasted_iota(jnp.int32, (n_ep, tok), 0)
    slots = lax.broadcasted_iota(jnp.int32, (cap, tok), 0)
    base = jnp.zeros((n_ep, 1), jnp.float32)
    for k in range(picks):
        ids = ids_ref[k : k + 1, :]
        mine = (ids >> shift) == owners
        hot = jnp.where(mine, 1.0, 0.0)
        rank = base + jnp.dot(
            hot.astype(jnp.bfloat16), before, preferred_element_type=jnp.float32
        )
        place = jnp.sum(jnp.where(mine, rank, 0.0), axis=0, keepdims=True).astype(jnp.int32)
        base = base + jnp.sum(hot, axis=1, keepdims=True)
        b_ref[:, k * tok : (k + 1) * tok] = jnp.where(slots == place, 1.0, 0.0).astype(
            jnp.bfloat16
        )
        local = ids & ((1 << shift) - 1)
        gate = gates_ref[k : k + 1, :]
        gate_hi = gate.astype(jnp.bfloat16).astype(jnp.float32)
        gate_mid = (gate - gate_hi).astype(jnp.bfloat16).astype(jnp.float32)
        gate_lo = gate - gate_hi - gate_mid
        values = (
            token_no,
            (local >> 4).astype(jnp.float32),
            (local & 15).astype(jnp.float32),
            gate_hi,
            gate_mid,
            gate_lo,
        )
        for c, value in enumerate(values):
            a_ref[c * n_ep : (c + 1) * n_ep, k * tok : (k + 1) * tok] = jnp.where(
                mine, value, 0.0
            ).astype(jnp.bfloat16)
    res = lax.dot_general(
        a_ref[...], b_ref[...], (((1,), (1,)), ((), ())), preferred_element_type=jnp.float32
    )
    part = [res[c * n_ep : (c + 1) * n_ep] for c in range(6)]
    code = part[0] * float(1 << shift) + (part[1] * 16.0 + part[2])
    gates = part[3] + part[4] + part[5]
    chunks = cap // LANES
    out_ref[...] = jnp.zeros(out_ref.shape, jnp.float32)
    for j in range(chunks):
        out_ref[:, j, :] = code[:, j * LANES : (j + 1) * LANES]
        out_ref[:, chunks + j, :] = gates[:, j * LANES : (j + 1) * LANES]


def widen(table_ref, wide_ref):
    step = 256

    def one(i, carry):
        rows = pl.ds(pl.multiple_of(i * step, step), step)
        wide_ref[rows, :] = table_ref[rows, :].astype(jnp.float32)
        return carry

    lax.fori_loop(0, table_ref.shape[0] // step, one, 0)


def take_rows(rows_ref, line, wide_ref, picked, out_ref, to):
    for s in range(LANES):
        picked[pl.ds(s, 1), :] = wide_ref[pl.ds(rows_ref[line, s], 1), :]
    out_ref[to] = picked[...].astype(out_ref.dtype)


def chunks_of(count):
    return (count + LANES - 1) // LANES


def pick_kernel(
    x_ref,
    rows_ref,
    count_ref,
    place_ref,
    gate_ref,
    key_ref,
    value_ref,
    count_out,
    place_out,
    gate_out,
    keys_out,
    values_out,
    wide_k,
    wide_v,
    took_k,
    took_v,
):
    n_ep = count_ref.shape[0]
    n_z = n_ep // X
    chunks = place_ref.shape[0] // n_ep
    widen(key_ref, wide_k)
    widen(value_ref, wide_v)

    def block(i, carry):
        z = i // X
        shift = (x_ref[0] + X - i % X) % X
        slot = (shift // 2 + (shift % 2) * 2) * n_z + z
        count_out[slot] = count_ref[i]
        for c in range(chunks):
            place_out[pl.ds(slot * chunks + c, 1), :] = place_ref[pl.ds(i * chunks + c, 1), :]
            gate_out[pl.ds(slot * chunks + c, 1), :] = gate_ref[pl.ds(i * chunks + c, 1), :]

        def chunk(c, inner):
            take_rows(rows_ref, i * chunks + c, wide_k, took_k, keys_out, slot * chunks + c)
            take_rows(rows_ref, i * chunks + c, wide_v, took_v, values_out, slot * chunks + c)
            return inner

        lax.fori_loop(0, chunks_of(count_ref[i]), chunk, 0)
        return carry

    lax.fori_loop(0, n_ep, block, 0)


def score_kernel(count_ref, place_ref, keys_ref, *refs, members):
    toks = dict(zip(members, refs))
    out_ref = refs[-1]
    n_z, tok, _ = refs[0].shape
    chunks = place_ref.shape[0] // (X * n_z)
    if len(refs) > len(members) + 1:
        out_ref[...] = refs[-2][...]
    else:
        out_ref[...] = jnp.zeros(out_ref.shape, jnp.float32)
    token_of = lax.broadcasted_iota(jnp.int32, (tok, LANES), 0)

    def line_scores(tokens, line):
        prod = lax.dot_general(
            tokens, keys_ref[line], (((1,), (1,)), ((), ())), preferred_element_type=jnp.float32
        )
        here = place_ref[pl.ds(line, 1), :] == token_of
        return jnp.sum(jnp.where(here, prod, 0.0), axis=0, keepdims=True)

    per = 4 // len(members) if 4 % len(members) == 0 else 1

    def first(step, carry):
        jobs = [(g, step * per + j) for j in range(per) for g in members]
        found = [line_scores(toks[g][z], (g * n_z + z) * chunks) for g, z in jobs]
        for (g, z), value in zip(jobs, found):
            out_ref[pl.ds((g * n_z + z) * chunks, 1), :] = value
        return carry

    lax.fori_loop(0, n_z // per, first, 0)

    def more(z, carry):
        for g in members:

            def chunk(c, inner, g=g):
                line = (g * n_z + z) * chunks + c
                out_ref[pl.ds(line, 1), :] = line_scores(toks[g][z], line)
                return inner

            lax.fori_loop(1, chunks_of(count_ref[g * n_z + z]), chunk, 0)
        return carry

    lax.fori_loop(0, n_z, more, 0)


def combine_kernel(count_ref, place_ref, hidden_ref, values_ref, out_ref, acc, *, group):
    n_z, tok, _ = out_ref.shape
    chunks = place_ref.shape[0] // (X * n_z)
    token_of = lax.broadcasted_iota(jnp.int32, (tok, LANES), 0)

    def line_mix(z, c):
        line = (group * n_z + z) * chunks + c
        here = place_ref[pl.ds(line, 1), :] == token_of
        weight = jnp.where(here, hidden_ref[pl.ds(line, 1), :], 0.0)
        high = weight.astype(jnp.bfloat16)
        low = (weight - high.astype(jnp.float32)).astype(jnp.bfloat16)
        rows = values_ref[line]
        return jnp.dot(
            jnp.concatenate([high, low], axis=1),
            jnp.concatenate([rows, rows], axis=0),
            preferred_element_type=jnp.float32,
        )

    def first(half, carry):
        zs = [half * 4 + j for j in range(4)]
        found = [line_mix(z, 0) for z in zs]
        for z, value in zip(zs, found):
            acc[z] = value
        return carry

    lax.fori_loop(0, n_z // 4, first, 0)

    def more(z, carry):
        def chunk(c, inner):
            acc[z] += line_mix(z, c)
            return inner

        lax.fori_loop(1, chunks_of(count_ref[group * n_z + z]), chunk, 0)
        out_ref[z] = acc[z].astype(out_ref.dtype)
        return carry

    lax.fori_loop(0, n_z, more, 0)


def vmem():
    return pl.BlockSpec(memory_space=pltpu.VMEM)


def made(shape, dtype):
    return jax.ShapeDtypeStruct(shape, dtype) if INTERPRET else pltpu.VMEM(shape, dtype)


def held(value, where=pltpu.VMEM):
    return value if INTERPRET else pltpu.with_memory_space_constraint(value, where)


def smem():
    return pl.BlockSpec(memory_space=pltpu.SMEM)


def to_each(value, axis):
    return lax.all_to_all(
        jnp.broadcast_to(value[None], (lax.axis_size(axis), *value.shape)), axis, 0, 0, tiled=True
    )


def around(shift):
    return [(i, (i + shift) % X) for i in range(X)]


def body(tokens, row_ids, row_gates, key_table, value_table, norm_gain):
    tok, width = tokens.shape
    picks = row_ids.shape[1]
    exp_dev = key_table.shape[0]
    n_ep = lax.axis_size(EP)
    cap = 3 * tok * picks // n_ep
    chunks = cap // LANES
    shift = exp_dev.bit_length() - 1
    lines = n_ep * chunks

    near = to_each(tokens, "z")
    groups = [near]
    for g in (1, 2, 3):
        groups.append(lax.ppermute(near, "x", around(SHIFTS[g])))
    listed = pl.pallas_call(
        lambda *refs: bucket_kernel(*refs, n_ep=n_ep, cap=cap, shift=shift),
        out_shape=jax.ShapeDtypeStruct((n_ep, 8, LANES), jnp.float32),
        in_specs=[vmem(), vmem()],
        out_specs=vmem(),
        scratch_shapes=[
            pltpu.VMEM((6 * n_ep, tok * picks), jnp.bfloat16),
            pltpu.VMEM((cap, tok * picks), jnp.bfloat16),
        ],
        interpret=INTERPRET,
        compiler_params=pltpu.CompilerParams(vmem_limit_bytes=ROOM),
        name="bucket",
    )(row_ids.T, row_gates.T)
    listed = lax.all_to_all(listed, EP, 0, 0, tiled=True)
    codes = listed[:, :chunks].astype(jnp.int32)
    gates = listed[:, chunks : 2 * chunks].reshape(lines, LANES)
    rows = (codes & (exp_dev - 1)).reshape(lines, LANES)
    place = ((codes >> shift) - 1).reshape(lines, LANES)
    count = jnp.sum((codes > 0).astype(jnp.int32), axis=(1, 2))

    n_z = n_ep // X
    picked = made((lines, LANES, width), jnp.bfloat16)
    count, place, gates, keys, values = pl.pallas_call(
        pick_kernel,
        out_shape=(
            jax.ShapeDtypeStruct((n_ep,), jnp.int32),
            jax.ShapeDtypeStruct((lines, LANES), jnp.int32),
            jax.ShapeDtypeStruct((lines, LANES), jnp.float32),
            picked,
            picked,
        ),
        in_specs=[smem(), smem(), smem(), vmem(), vmem(), vmem(), vmem()],
        out_specs=(smem(), vmem(), vmem(), vmem(), vmem()),
        scratch_shapes=[
            pltpu.VMEM((exp_dev, width), jnp.float32),
            pltpu.VMEM((exp_dev, width), jnp.float32),
            pltpu.VMEM((LANES, width), jnp.float32),
            pltpu.VMEM((LANES, width), jnp.float32),
        ],
        interpret=INTERPRET,
        compiler_params=pltpu.CompilerParams(vmem_limit_bytes=ROOM),
        name="pick",
    )(
        lax.axis_index("x").reshape(1),
        rows,
        count,
        place,
        gates,
        held(key_table, pltpu.HBM),
        held(value_table, pltpu.HBM),
    )

    def scored(members, *before):
        toks = [held(groups[g]) for g in members]
        return pl.pallas_call(
            lambda *refs: score_kernel(*refs, members=members),
            out_shape=made((lines, LANES), jnp.float32),
            in_specs=[smem()] + [vmem()] * (2 + len(toks) + len(before)),
            out_specs=vmem(),
            interpret=INTERPRET,
            compiler_params=pltpu.CompilerParams(vmem_limit_bytes=ROOM),
            name="score",
        )(count, held(place), held(keys), *toks, *before)

    partial_score = scored((0, 1, 3))
    partial_score = scored((2,), held(partial_score))
    score = jnp.sum(lax.all_gather(partial_score, TP), axis=0)
    hidden = jnp.where(place >= 0, jax.nn.gelu(score, approximate=False) * gates, 0.0)

    def combine(group):
        return pl.pallas_call(
            lambda *refs: combine_kernel(*refs, group=group),
            out_shape=made((n_z, tok, width), jnp.bfloat16),
            in_specs=[smem(), vmem(), vmem(), vmem()],
            out_specs=vmem(),
            scratch_shapes=[pltpu.VMEM((n_z, tok, width), jnp.float32)],
            interpret=INTERPRET,
            compiler_params=pltpu.CompilerParams(vmem_limit_bytes=ROOM),
            name="combine",
        )(count, held(place), held(hidden), held(values))

    parts = []
    for g in (1, 2, 3, 0):
        part = combine(g)
        if g:
            part = lax.ppermute(part, "x", around(-SHIFTS[g]))
        parts.append(part)
    mine = sum(p.astype(jnp.float32) for p in parts).astype(jnp.bfloat16)
    back = lax.all_to_all(mine, "z", 0, 0, tiled=True)
    mixed = jnp.sum(back.astype(jnp.float32), axis=0)
    part = jnp.sum(mixed * mixed, axis=1).reshape(tok // LANES, LANES)
    squares = jnp.sum(to_each(part, TP), axis=0).reshape(tok)
    strength = squares / D
    return (mixed * lax.rsqrt(strength + 1e-06)[:, None] * norm_gain).astype(jnp.bfloat16)


def solution(mesh):
    ep, tp = mesh.devices.shape
    fine = Mesh(mesh.devices.reshape(Z, ep // Z, tp // 2, 2), ("z", "x", "y", "core"))
    in_specs = (P(EP, TP), P(EP, None), P(EP, None), P(EP, TP), P(EP, TP), P(TP))

    return jax.shard_map(body, mesh=fine, in_specs=in_specs, out_specs=P(EP, TP), check_vma=False)
```

```python
import jax
import jax.numpy as jnp
from jax import lax
from jax.experimental import pallas as pl
from jax.experimental.pallas import tpu as pltpu
from jax.sharding import Mesh
from jax.sharding import PartitionSpec as P

D = 2048
LANES = 128
INTERPRET = False
Z = 8
X = 4
ROOM = 24 * 1024 * 1024
SHIFTS = (0, 2, 1, 3)
EP = ("z", "x")
TP = ("y", "core")


def bucket_kernel(ids_ref, gates_ref, out_ref, a_ref, b_ref, *, n_ep, cap, shift):
    picks, tok = ids_ref.shape
    before = jnp.where(
        lax.broadcasted_iota(jnp.int32, (tok, tok), 0)
        < lax.broadcasted_iota(jnp.int32, (tok, tok), 1),
        1.0,
        0.0,
    ).astype(jnp.bfloat16)
    token_no = (lax.broadcasted_iota(jnp.int32, (1, tok), 1) + 1).astype(jnp.float32)
    owners = lax.broadcasted_iota(jnp.int32, (n_ep, tok), 0)
    slots = lax.broadcasted_iota(jnp.int32, (cap, tok), 0)
    base = jnp.zeros((n_ep, 1), jnp.float32)
    for k in range(picks):
        ids = ids_ref[k : k + 1, :]
        mine = (ids >> shift) == owners
        hot = jnp.where(mine, 1.0, 0.0)
        rank = base + jnp.dot(
            hot.astype(jnp.bfloat16), before, preferred_element_type=jnp.float32
        )
        place = jnp.sum(jnp.where(mine, rank, 0.0), axis=0, keepdims=True).astype(jnp.int32)
        base = base + jnp.sum(hot, axis=1, keepdims=True)
        b_ref[:, k * tok : (k + 1) * tok] = jnp.where(slots == place, 1.0, 0.0).astype(
            jnp.bfloat16
        )
        local = ids & ((1 << shift) - 1)
        gate = gates_ref[k : k + 1, :]
        gate_hi = gate.astype(jnp.bfloat16).astype(jnp.float32)
        gate_mid = (gate - gate_hi).astype(jnp.bfloat16).astype(jnp.float32)
        gate_lo = gate - gate_hi - gate_mid
        values = (
            token_no,
            (local >> 4).astype(jnp.float32),
            (local & 15).astype(jnp.float32),
            gate_hi,
            gate_mid,
            gate_lo,
        )
        for c, value in enumerate(values):
            a_ref[c * n_ep : (c + 1) * n_ep, k * tok : (k + 1) * tok] = jnp.where(
                mine, value, 0.0
            ).astype(jnp.bfloat16)
    res = lax.dot_general(
        a_ref[...], b_ref[...], (((1,), (1,)), ((), ())), preferred_element_type=jnp.float32
    )
    part = [res[c * n_ep : (c + 1) * n_ep] for c in range(6)]
    code = part[0] * float(1 << shift) + (part[1] * 16.0 + part[2])
    gates = part[3] + part[4] + part[5]
    chunks = cap // LANES
    out_ref[...] = jnp.zeros(out_ref.shape, jnp.float32)
    for j in range(chunks):
        out_ref[:, j, :] = code[:, j * LANES : (j + 1) * LANES]
        out_ref[:, chunks + j, :] = gates[:, j * LANES : (j + 1) * LANES]


def widen(table_ref, wide_ref, which):
    step = 256

    def one(i, carry):
        rows = pl.ds(pl.multiple_of(i * step, step), step)
        into = pl.ds(pl.multiple_of(i * 2 * step, 2 * step) + which, step, stride=2)
        wide_ref[into, :] = table_ref[rows, :].astype(jnp.float32)
        return carry

    lax.fori_loop(0, table_ref.shape[0] // step, one, 0)


def take_rows(rows_ref, line, wide_ref, picked, keys_out, values_out, to):
    for s in range(LANES):
        at = pl.multiple_of(rows_ref[line, s] * 2, 2)
        picked[pl.ds(2 * s, 2), :] = wide_ref[pl.ds(at, 2), :]
    keys_out[to] = picked[pl.ds(0, LANES, stride=2), :].astype(keys_out.dtype)
    values_out[to] = picked[pl.ds(1, LANES, stride=2), :].astype(values_out.dtype)


def chunks_of(count):
    return (count + LANES - 1) // LANES


def pick_kernel(
    x_ref,
    rows_ref,
    count_ref,
    place_ref,
    gate_ref,
    key_ref,
    value_ref,
    count_out,
    place_out,
    gate_out,
    keys_out,
    values_out,
    wide,
    took,
):
    n_ep = count_ref.shape[0]
    n_z = n_ep // X
    chunks = place_ref.shape[0] // n_ep
    widen(key_ref, wide, 0)
    widen(value_ref, wide, 1)

    def block(i, carry):
        z = i // X
        shift = (x_ref[0] + X - i % X) % X
        slot = (shift // 2 + (shift % 2) * 2) * n_z + z
        count_out[slot] = count_ref[i]
        for c in range(chunks):
            place_out[pl.ds(slot * chunks + c, 1), :] = place_ref[pl.ds(i * chunks + c, 1), :]
            gate_out[pl.ds(slot * chunks + c, 1), :] = gate_ref[pl.ds(i * chunks + c, 1), :]

        def chunk(c, inner):
            take_rows(
                rows_ref, i * chunks + c, wide, took, keys_out, values_out, slot * chunks + c
            )
            return inner

        lax.fori_loop(0, chunks_of(count_ref[i]), chunk, 0)
        return carry

    lax.fori_loop(0, n_ep, block, 0)


def score_kernel(count_ref, place_ref, keys_ref, *refs, members):
    toks = dict(zip(members, refs))
    out_ref = refs[-1]
    n_z, tok, _ = refs[0].shape
    chunks = place_ref.shape[0] // (X * n_z)
    if len(refs) > len(members) + 1:
        out_ref[...] = refs[-2][...]
    else:
        out_ref[...] = jnp.zeros(out_ref.shape, jnp.float32)
    token_of = lax.broadcasted_iota(jnp.int32, (tok, LANES), 0)

    def line_scores(tokens, line):
        prod = lax.dot_general(
            tokens, keys_ref[line], (((1,), (1,)), ((), ())), preferred_element_type=jnp.float32
        )
        here = place_ref[pl.ds(line, 1), :] == token_of
        return jnp.sum(jnp.where(here, prod, 0.0), axis=0, keepdims=True)

    per = 4 // len(members) if 4 % len(members) == 0 else 1

    def first(step, carry):
        jobs = [(g, step * per + j) for j in range(per) for g in members]
        found = [line_scores(toks[g][z], (g * n_z + z) * chunks) for g, z in jobs]
        for (g, z), value in zip(jobs, found):
            out_ref[pl.ds((g * n_z + z) * chunks, 1), :] = value
        return carry

    lax.fori_loop(0, n_z // per, first, 0)

    def more(z, carry):
        for g in members:

            def chunk(c, inner, g=g):
                line = (g * n_z + z) * chunks + c
                out_ref[pl.ds(line, 1), :] = line_scores(toks[g][z], line)
                return inner

            lax.fori_loop(1, chunks_of(count_ref[g * n_z + z]), chunk, 0)
        return carry

    lax.fori_loop(0, n_z, more, 0)


def combine_kernel(count_ref, place_ref, hidden_ref, values_ref, out_ref, acc, *, group):
    n_z, tok, _ = out_ref.shape
    chunks = place_ref.shape[0] // (X * n_z)
    token_of = lax.broadcasted_iota(jnp.int32, (tok, LANES), 0)

    def line_mix(z, c):
        line = (group * n_z + z) * chunks + c
        here = place_ref[pl.ds(line, 1), :] == token_of
        weight = jnp.where(here, hidden_ref[pl.ds(line, 1), :], 0.0)
        high = weight.astype(jnp.bfloat16)
        low = (weight - high.astype(jnp.float32)).astype(jnp.bfloat16)
        rows = values_ref[line]
        return jnp.dot(
            jnp.concatenate([high, low], axis=1),
            jnp.concatenate([rows, rows], axis=0),
            preferred_element_type=jnp.float32,
        )

    def first(half, carry):
        zs = [half * 4 + j for j in range(4)]
        found = [line_mix(z, 0) for z in zs]
        for z, value in zip(zs, found):
            acc[z] = value
        return carry

    lax.fori_loop(0, n_z // 4, first, 0)

    def more(z, carry):
        def chunk(c, inner):
            acc[z] += line_mix(z, c)
            return inner

        lax.fori_loop(1, chunks_of(count_ref[group * n_z + z]), chunk, 0)
        out_ref[z] = acc[z].astype(out_ref.dtype)
        return carry

    lax.fori_loop(0, n_z, more, 0)


def vmem():
    return pl.BlockSpec(memory_space=pltpu.VMEM)


def made(shape, dtype):
    return jax.ShapeDtypeStruct(shape, dtype) if INTERPRET else pltpu.VMEM(shape, dtype)


def held(value, where=pltpu.VMEM):
    return value if INTERPRET else pltpu.with_memory_space_constraint(value, where)


def smem():
    return pl.BlockSpec(memory_space=pltpu.SMEM)


def to_each(value, axis):
    return lax.all_to_all(
        jnp.broadcast_to(value[None], (lax.axis_size(axis), *value.shape)), axis, 0, 0, tiled=True
    )


def around(shift):
    return [(i, (i + shift) % X) for i in range(X)]


def body(tokens, row_ids, row_gates, key_table, value_table, norm_gain):
    tok, width = tokens.shape
    picks = row_ids.shape[1]
    exp_dev = key_table.shape[0]
    n_ep = lax.axis_size(EP)
    cap = 3 * tok * picks // n_ep
    chunks = cap // LANES
    shift = exp_dev.bit_length() - 1
    lines = n_ep * chunks

    near = to_each(tokens, "z")
    groups = [near]
    for g in (1, 2, 3):
        groups.append(lax.ppermute(near, "x", around(SHIFTS[g])))
    listed = pl.pallas_call(
        lambda *refs: bucket_kernel(*refs, n_ep=n_ep, cap=cap, shift=shift),
        out_shape=jax.ShapeDtypeStruct((n_ep, 8, LANES), jnp.float32),
        in_specs=[vmem(), vmem()],
        out_specs=vmem(),
        scratch_shapes=[
            pltpu.VMEM((6 * n_ep, tok * picks), jnp.bfloat16),
            pltpu.VMEM((cap, tok * picks), jnp.bfloat16),
        ],
        interpret=INTERPRET,
        compiler_params=pltpu.CompilerParams(vmem_limit_bytes=ROOM),
        name="bucket",
    )(row_ids.T, row_gates.T)
    listed = lax.all_to_all(listed, EP, 0, 0, tiled=True)
    codes = listed[:, :chunks].astype(jnp.int32)
    gates = listed[:, chunks : 2 * chunks].reshape(lines, LANES)
    rows = (codes & (exp_dev - 1)).reshape(lines, LANES)
    place = ((codes >> shift) - 1).reshape(lines, LANES)
    count = jnp.sum((codes > 0).astype(jnp.int32), axis=(1, 2))

    n_z = n_ep // X
    picked = made((lines, LANES, width), jnp.bfloat16)
    count, place, gates, keys, values = pl.pallas_call(
        pick_kernel,
        out_shape=(
            jax.ShapeDtypeStruct((n_ep,), jnp.int32),
            jax.ShapeDtypeStruct((lines, LANES), jnp.int32),
            jax.ShapeDtypeStruct((lines, LANES), jnp.float32),
            picked,
            picked,
        ),
        in_specs=[smem(), smem(), smem(), vmem(), vmem(), vmem(), vmem()],
        out_specs=(smem(), vmem(), vmem(), vmem(), vmem()),
        scratch_shapes=[
            pltpu.VMEM((2 * exp_dev, width), jnp.float32),
            pltpu.VMEM((2 * LANES, width), jnp.float32),
        ],
        interpret=INTERPRET,
        compiler_params=pltpu.CompilerParams(vmem_limit_bytes=ROOM),
        name="pick",
    )(
        lax.axis_index("x").reshape(1),
        rows,
        count,
        place,
        gates,
        held(key_table, pltpu.HBM),
        held(value_table, pltpu.HBM),
    )

    def scored(members, *before):
        toks = [held(groups[g]) for g in members]
        return pl.pallas_call(
            lambda *refs: score_kernel(*refs, members=members),
            out_shape=made((lines, LANES), jnp.float32),
            in_specs=[smem()] + [vmem()] * (2 + len(toks) + len(before)),
            out_specs=vmem(),
            interpret=INTERPRET,
            compiler_params=pltpu.CompilerParams(vmem_limit_bytes=ROOM),
            name="score",
        )(count, held(place), held(keys), *toks, *before)

    partial_score = scored((0, 1, 3))
    partial_score = scored((2,), held(partial_score))
    score = jnp.sum(lax.all_gather(partial_score, TP), axis=0)
    hidden = jnp.where(place >= 0, jax.nn.gelu(score, approximate=False) * gates, 0.0)

    def combine(group):
        return pl.pallas_call(
            lambda *refs: combine_kernel(*refs, group=group),
            out_shape=made((n_z, tok, width), jnp.bfloat16),
            in_specs=[smem(), vmem(), vmem(), vmem()],
            out_specs=vmem(),
            scratch_shapes=[pltpu.VMEM((n_z, tok, width), jnp.float32)],
            interpret=INTERPRET,
            compiler_params=pltpu.CompilerParams(vmem_limit_bytes=ROOM),
            name="combine",
        )(count, held(place), held(hidden), held(values))

    parts = []
    for g in (1, 2, 3, 0):
        part = combine(g)
        if g:
            part = lax.ppermute(part, "x", around(-SHIFTS[g]))
        parts.append(part)
    mine = sum(p.astype(jnp.float32) for p in parts).astype(jnp.bfloat16)
    back = lax.all_to_all(mine, "z", 0, 0, tiled=True)
    mixed = jnp.sum(back.astype(jnp.float32), axis=0)
    part = jnp.sum(mixed * mixed, axis=1).reshape(tok // LANES, LANES)
    squares = jnp.sum(to_each(part, TP), axis=0).reshape(tok)
    strength = squares / D
    return (mixed * lax.rsqrt(strength + 1e-06)[:, None] * norm_gain).astype(jnp.bfloat16)


def solution(mesh):
    ep, tp = mesh.devices.shape
    fine = Mesh(mesh.devices.reshape(Z, ep // Z, tp // 2, 2), ("z", "x", "y", "core"))
    in_specs = (P(EP, TP), P(EP, None), P(EP, None), P(EP, TP), P(EP, TP), P(TP))

    return jax.shard_map(body, mesh=fine, in_specs=in_specs, out_specs=P(EP, TP), check_vma=False)
```

```python
import jax
import jax.numpy as jnp
from jax import lax
from jax.experimental import pallas as pl
from jax.experimental.pallas import tpu as pltpu
from jax.sharding import Mesh
from jax.sharding import PartitionSpec as P

D = 2048
LANES = 128
INTERPRET = False
Z = 8
X = 4
ROOM = 24 * 1024 * 1024
SHIFTS = (0, 2, 1, 3)
EP = ("z", "x")
TP = ("y", "core")


def bucket_kernel(ids_ref, gates_ref, out_ref, a_ref, b_ref, *, n_ep, cap, shift):
    picks, tok = ids_ref.shape
    before = jnp.where(
        lax.broadcasted_iota(jnp.int32, (tok, tok), 0)
        < lax.broadcasted_iota(jnp.int32, (tok, tok), 1),
        1.0,
        0.0,
    ).astype(jnp.bfloat16)
    token_no = (lax.broadcasted_iota(jnp.int32, (1, tok), 1) + 1).astype(jnp.float32)
    owners = lax.broadcasted_iota(jnp.int32, (n_ep, tok), 0)
    slots = lax.broadcasted_iota(jnp.int32, (cap, tok), 0)
    base = jnp.zeros((n_ep, 1), jnp.float32)
    for k in range(picks):
        ids = ids_ref[k : k + 1, :]
        mine = (ids >> shift) == owners
        hot = jnp.where(mine, 1.0, 0.0)
        rank = base + jnp.dot(
            hot.astype(jnp.bfloat16), before, preferred_element_type=jnp.float32
        )
        place = jnp.sum(jnp.where(mine, rank, 0.0), axis=0, keepdims=True).astype(jnp.int32)
        base = base + jnp.sum(hot, axis=1, keepdims=True)
        b_ref[:, k * tok : (k + 1) * tok] = jnp.where(slots == place, 1.0, 0.0).astype(
            jnp.bfloat16
        )
        local = ids & ((1 << shift) - 1)
        gate = gates_ref[k : k + 1, :]
        gate_hi = gate.astype(jnp.bfloat16).astype(jnp.float32)
        gate_mid = (gate - gate_hi).astype(jnp.bfloat16).astype(jnp.float32)
        gate_lo = gate - gate_hi - gate_mid
        values = (
            token_no,
            (local >> 4).astype(jnp.float32),
            (local & 15).astype(jnp.float32),
            gate_hi,
            gate_mid,
            gate_lo,
        )
        for c, value in enumerate(values):
            a_ref[c * n_ep : (c + 1) * n_ep, k * tok : (k + 1) * tok] = jnp.where(
                mine, value, 0.0
            ).astype(jnp.bfloat16)
    res = lax.dot_general(
        a_ref[...], b_ref[...], (((1,), (1,)), ((), ())), preferred_element_type=jnp.float32
    )
    part = [res[c * n_ep : (c + 1) * n_ep] for c in range(6)]
    code = part[0] * float(1 << shift) + (part[1] * 16.0 + part[2])
    gates = part[3] + part[4] + part[5]
    chunks = cap // LANES
    out_ref[...] = jnp.zeros(out_ref.shape, jnp.float32)
    for j in range(chunks):
        out_ref[:, j, :] = code[:, j * LANES : (j + 1) * LANES]
        out_ref[:, chunks + j, :] = gates[:, j * LANES : (j + 1) * LANES]


def widen(table_ref, wide_ref, which):
    step = 256

    def one(i, carry):
        rows = pl.ds(pl.multiple_of(i * step, step), step)
        into = pl.ds(pl.multiple_of(i * 2 * step, 2 * step) + which, step, stride=2)
        wide_ref[into, :] = table_ref[rows, :].astype(jnp.float32)
        return carry

    lax.fori_loop(0, table_ref.shape[0] // step, one, 0)


def take_rows(rows_ref, line, wide_ref, picked, keys_out, values_out, to):
    for s in range(LANES):
        at = pl.multiple_of(rows_ref[line, s], 2)
        picked[pl.ds(2 * s, 2), :] = wide_ref[pl.ds(at, 2), :]
    keys_out[to] = picked[pl.ds(0, LANES, stride=2), :].astype(keys_out.dtype)
    values_out[to] = picked[pl.ds(1, LANES, stride=2), :].astype(values_out.dtype)


def repeat_kernel(tok_ref, out_ref):
    for i in range(out_ref.shape[0]):
        out_ref[i] = tok_ref[...]


def chunks_of(count):
    return (count + LANES - 1) // LANES


def pick_kernel(
    x_ref,
    rows_ref,
    count_ref,
    place_ref,
    gate_ref,
    key_ref,
    value_ref,
    count_out,
    place_out,
    gate_out,
    keys_out,
    values_out,
    wide,
    took,
):
    n_ep = count_ref.shape[0]
    n_z = n_ep // X
    chunks = place_ref.shape[0] // n_ep
    widen(key_ref, wide, 0)
    widen(value_ref, wide, 1)

    def block(i, carry):
        z = i // X
        shift = (x_ref[0] + X - i % X) % X
        slot = (shift // 2 + (shift % 2) * 2) * n_z + z
        count_out[slot] = count_ref[i]
        for c in range(chunks):
            place_out[pl.ds(slot * chunks + c, 1), :] = place_ref[pl.ds(i * chunks + c, 1), :]
            gate_out[pl.ds(slot * chunks + c, 1), :] = gate_ref[pl.ds(i * chunks + c, 1), :]

        def chunk(c, inner):
            take_rows(
                rows_ref, i * chunks + c, wide, took, keys_out, values_out, slot * chunks + c
            )
            return inner

        lax.fori_loop(0, chunks_of(count_ref[i]), chunk, 0)
        return carry

    lax.fori_loop(0, n_ep, block, 0)


def score_kernel(count_ref, place_ref, keys_ref, *refs, members):
    toks = dict(zip(members, refs))
    out_ref = refs[-1]
    n_z, tok, _ = refs[0].shape
    chunks = place_ref.shape[0] // (X * n_z)
    if len(refs) > len(members) + 1:
        out_ref[...] = refs[-2][...]
    else:
        out_ref[...] = jnp.zeros(out_ref.shape, jnp.float32)
    token_of = lax.broadcasted_iota(jnp.int32, (tok, LANES), 0)

    def line_scores(tokens, line):
        prod = lax.dot_general(
            tokens, keys_ref[line], (((1,), (1,)), ((), ())), preferred_element_type=jnp.float32
        )
        here = place_ref[pl.ds(line, 1), :] == token_of
        return jnp.sum(jnp.where(here, prod, 0.0), axis=0, keepdims=True)

    per = 4 if len(members) == 1 else 2

    def first(step, carry):
        jobs = [(g, step * per + j) for j in range(per) for g in members]
        found = [line_scores(toks[g][z], (g * n_z + z) * chunks) for g, z in jobs]
        for (g, z), value in zip(jobs, found):
            out_ref[pl.ds((g * n_z + z) * chunks, 1), :] = value
        return carry

    lax.fori_loop(0, n_z // per, first, 0)

    def more(z, carry):
        for g in members:

            def chunk(c, inner, g=g):
                line = (g * n_z + z) * chunks + c
                out_ref[pl.ds(line, 1), :] = line_scores(toks[g][z], line)
                return inner

            lax.fori_loop(1, chunks_of(count_ref[g * n_z + z]), chunk, 0)
        return carry

    lax.fori_loop(0, n_z, more, 0)


def combine_kernel(count_ref, place_ref, hidden_ref, values_ref, out_ref, acc, *, group):
    n_z, tok, _ = out_ref.shape
    chunks = place_ref.shape[0] // (X * n_z)
    token_of = lax.broadcasted_iota(jnp.int32, (tok, LANES), 0)

    def line_mix(z, c):
        line = (group * n_z + z) * chunks + c
        here = place_ref[pl.ds(line, 1), :] == token_of
        weight = jnp.where(here, hidden_ref[pl.ds(line, 1), :], 0.0)
        high = weight.astype(jnp.bfloat16)
        low = (weight - high.astype(jnp.float32)).astype(jnp.bfloat16)
        rows = values_ref[line]
        return jnp.dot(
            jnp.concatenate([high, low], axis=1),
            jnp.concatenate([rows, rows], axis=0),
            preferred_element_type=jnp.float32,
        )

    def first(half, carry):
        zs = [half * 4 + j for j in range(4)]
        found = [line_mix(z, 0) for z in zs]
        for z, value in zip(zs, found):
            acc[z] = value
        return carry

    lax.fori_loop(0, n_z // 4, first, 0)

    def more(z, carry):
        def chunk(c, inner):
            acc[z] += line_mix(z, c)
            return inner

        lax.fori_loop(1, chunks_of(count_ref[group * n_z + z]), chunk, 0)
        out_ref[z] = acc[z].astype(out_ref.dtype)
        return carry

    lax.fori_loop(0, n_z, more, 0)


def vmem():
    return pl.BlockSpec(memory_space=pltpu.VMEM)


def made(shape, dtype):
    return jax.ShapeDtypeStruct(shape, dtype) if INTERPRET else pltpu.VMEM(shape, dtype)


def held(value, where=pltpu.VMEM):
    return value if INTERPRET else pltpu.with_memory_space_constraint(value, where)


def smem():
    return pl.BlockSpec(memory_space=pltpu.SMEM)


def to_each(value, axis):
    return lax.all_to_all(
        jnp.broadcast_to(value[None], (lax.axis_size(axis), *value.shape)), axis, 0, 0, tiled=True
    )


def around(shift):
    return [(i, (i + shift) % X) for i in range(X)]


def body(tokens, row_ids, row_gates, key_table, value_table, norm_gain):
    tok, width = tokens.shape
    picks = row_ids.shape[1]
    exp_dev = key_table.shape[0]
    n_ep = lax.axis_size(EP)
    cap = 3 * tok * picks // n_ep
    chunks = cap // LANES
    shift = exp_dev.bit_length() - 1
    lines = n_ep * chunks

    copies = pl.pallas_call(
        repeat_kernel,
        out_shape=made((lax.axis_size("z"), tok, width), tokens.dtype),
        in_specs=[vmem()],
        out_specs=vmem(),
        interpret=INTERPRET,
        compiler_params=pltpu.CompilerParams(vmem_limit_bytes=ROOM),
        name="repeat",
    )(held(tokens, pltpu.HBM))
    near = lax.all_to_all(copies, "z", 0, 0, tiled=True)
    groups = [near]
    for g in (1, 2, 3):
        groups.append(lax.ppermute(near, "x", around(SHIFTS[g])))
    listed = pl.pallas_call(
        lambda *refs: bucket_kernel(*refs, n_ep=n_ep, cap=cap, shift=shift),
        out_shape=jax.ShapeDtypeStruct((n_ep, 8, LANES), jnp.float32),
        in_specs=[vmem(), vmem()],
        out_specs=vmem(),
        scratch_shapes=[
            pltpu.VMEM((6 * n_ep, tok * picks), jnp.bfloat16),
            pltpu.VMEM((cap, tok * picks), jnp.bfloat16),
        ],
        interpret=INTERPRET,
        compiler_params=pltpu.CompilerParams(vmem_limit_bytes=ROOM),
        name="bucket",
    )(row_ids.T, row_gates.T)
    listed = lax.all_to_all(listed, EP, 0, 0, tiled=True)
    codes = listed[:, :chunks].astype(jnp.int32)
    gates = listed[:, chunks : 2 * chunks].reshape(lines, LANES)
    rows = ((codes & (exp_dev - 1)) * 2).reshape(lines, LANES)
    place = ((codes >> shift) - 1).reshape(lines, LANES)
    count = jnp.sum((codes > 0).astype(jnp.int32), axis=(1, 2))

    n_z = n_ep // X
    picked = made((lines, LANES, width), jnp.bfloat16)
    count, place, gates, keys, values = pl.pallas_call(
        pick_kernel,
        out_shape=(
            jax.ShapeDtypeStruct((n_ep,), jnp.int32),
            jax.ShapeDtypeStruct((lines, LANES), jnp.int32),
            jax.ShapeDtypeStruct((lines, LANES), jnp.float32),
            picked,
            picked,
        ),
        in_specs=[smem(), smem(), smem(), vmem(), vmem(), vmem(), vmem()],
        out_specs=(smem(), vmem(), vmem(), vmem(), vmem()),
        scratch_shapes=[
            pltpu.VMEM((2 * exp_dev, width), jnp.float32),
            pltpu.VMEM((2 * LANES, width), jnp.float32),
        ],
        interpret=INTERPRET,
        compiler_params=pltpu.CompilerParams(vmem_limit_bytes=ROOM),
        name="pick",
    )(
        lax.axis_index("x").reshape(1),
        rows,
        count,
        place,
        gates,
        held(key_table, pltpu.HBM),
        held(value_table, pltpu.HBM),
    )

    def scored(members, *before):
        toks = [held(groups[g]) for g in members]
        return pl.pallas_call(
            lambda *refs: score_kernel(*refs, members=members),
            out_shape=made((lines, LANES), jnp.float32),
            in_specs=[smem()] + [vmem()] * (2 + len(toks) + len(before)),
            out_specs=vmem(),
            interpret=INTERPRET,
            compiler_params=pltpu.CompilerParams(vmem_limit_bytes=ROOM),
            name="score",
        )(count, held(place), held(keys), *toks, *before)

    partial_score = scored((0, 1, 3))
    partial_score = scored((2,), held(partial_score))
    score = jnp.sum(lax.all_gather(partial_score, TP), axis=0)
    hidden = jnp.where(place >= 0, jax.nn.gelu(score, approximate=False) * gates, 0.0)

    def combine(group):
        return pl.pallas_call(
            lambda *refs: combine_kernel(*refs, group=group),
            out_shape=made((n_z, tok, width), jnp.bfloat16),
            in_specs=[smem(), vmem(), vmem(), vmem()],
            out_specs=vmem(),
            scratch_shapes=[pltpu.VMEM((n_z, tok, width), jnp.float32)],
            interpret=INTERPRET,
            compiler_params=pltpu.CompilerParams(vmem_limit_bytes=ROOM),
            name="combine",
        )(count, held(place), held(hidden), held(values))

    parts = []
    for g in (1, 2, 3, 0):
        part = combine(g)
        if g:
            part = lax.ppermute(part, "x", around(-SHIFTS[g]))
        parts.append(part)
    mine = sum(p.astype(jnp.float32) for p in parts).astype(jnp.bfloat16)
    back = lax.all_to_all(mine, "z", 0, 0, tiled=True)
    mixed = jnp.sum(back.astype(jnp.float32), axis=0)
    part = jnp.sum(mixed * mixed, axis=1).reshape(tok // LANES, LANES)
    squares = jnp.sum(to_each(part, TP), axis=0).reshape(tok)
    strength = squares / D
    return (mixed * lax.rsqrt(strength + 1e-06)[:, None] * norm_gain).astype(jnp.bfloat16)


def solution(mesh):
    ep, tp = mesh.devices.shape
    fine = Mesh(mesh.devices.reshape(Z, ep // Z, tp // 2, 2), ("z", "x", "y", "core"))
    in_specs = (P(EP, TP), P(EP, None), P(EP, None), P(EP, TP), P(EP, TP), P(TP))

    return jax.shard_map(body, mesh=fine, in_specs=in_specs, out_specs=P(EP, TP), check_vma=False)
```

```python
import jax
import jax.numpy as jnp
from jax import lax
from jax.experimental import pallas as pl
from jax.experimental.pallas import tpu as pltpu
from jax.sharding import Mesh
from jax.sharding import PartitionSpec as P

D = 2048
LANES = 128
INTERPRET = False
Z = 8
X = 4
ROOM = 24 * 1024 * 1024
SHIFTS = (0, 2, 1, 3)
EP = ("z", "x")
TP = ("y", "core")


def bucket_kernel(ids_ref, gates_ref, out_ref, a_ref, b_ref, *, n_ep, cap, shift):
    picks, tok = ids_ref.shape
    before = jnp.where(
        lax.broadcasted_iota(jnp.int32, (tok, tok), 0)
        < lax.broadcasted_iota(jnp.int32, (tok, tok), 1),
        1.0,
        0.0,
    ).astype(jnp.bfloat16)
    token_no = (lax.broadcasted_iota(jnp.int32, (1, tok), 1) + 1).astype(jnp.float32)
    owners = lax.broadcasted_iota(jnp.int32, (n_ep, tok), 0)
    slots = lax.broadcasted_iota(jnp.int32, (cap, tok), 0)
    base = jnp.zeros((n_ep, 1), jnp.float32)
    for k in range(picks):
        ids = ids_ref[k : k + 1, :]
        mine = (ids >> shift) == owners
        hot = jnp.where(mine, 1.0, 0.0)
        rank = base + jnp.dot(
            hot.astype(jnp.bfloat16), before, preferred_element_type=jnp.float32
        )
        place = jnp.sum(jnp.where(mine, rank, 0.0), axis=0, keepdims=True).astype(jnp.int32)
        base = base + jnp.sum(hot, axis=1, keepdims=True)
        b_ref[:, k * tok : (k + 1) * tok] = jnp.where(slots == place, 1.0, 0.0).astype(
            jnp.bfloat16
        )
        local = ids & ((1 << shift) - 1)
        gate = gates_ref[k : k + 1, :]
        gate_hi = gate.astype(jnp.bfloat16).astype(jnp.float32)
        gate_mid = (gate - gate_hi).astype(jnp.bfloat16).astype(jnp.float32)
        gate_lo = gate - gate_hi - gate_mid
        values = (
            token_no,
            (local >> 4).astype(jnp.float32),
            (local & 15).astype(jnp.float32),
            gate_hi,
            gate_mid,
            gate_lo,
        )
        for c, value in enumerate(values):
            a_ref[c * n_ep : (c + 1) * n_ep, k * tok : (k + 1) * tok] = jnp.where(
                mine, value, 0.0
            ).astype(jnp.bfloat16)
    res = lax.dot_general(
        a_ref[...], b_ref[...], (((1,), (1,)), ((), ())), preferred_element_type=jnp.float32
    )
    part = [res[c * n_ep : (c + 1) * n_ep] for c in range(6)]
    code = part[0] * float(1 << shift) + (part[1] * 16.0 + part[2])
    gates = part[3] + part[4] + part[5]
    chunks = cap // LANES
    out_ref[...] = jnp.zeros(out_ref.shape, jnp.float32)
    for j in range(chunks):
        out_ref[:, j, :] = code[:, j * LANES : (j + 1) * LANES]
        out_ref[:, chunks + j, :] = gates[:, j * LANES : (j + 1) * LANES]


def widen(table_ref, wide_ref, which):
    step = 256

    def one(i, carry):
        rows = pl.ds(pl.multiple_of(i * step, step), step)
        into = pl.ds(pl.multiple_of(i * 2 * step, 2 * step) + which, step, stride=2)
        wide_ref[into, :] = table_ref[rows, :].astype(jnp.float32)
        return carry

    lax.fori_loop(0, table_ref.shape[0] // step, one, 0)


def take_rows(rows_ref, line, wide_ref, picked, keys_out, values_out, to):
    for s in range(LANES):
        at = pl.multiple_of(rows_ref[line, s], 2)
        picked[pl.ds(2 * s, 2), :] = wide_ref[pl.ds(at, 2), :]
    keys_out[to] = picked[pl.ds(0, LANES, stride=2), :].astype(keys_out.dtype)
    values_out[to] = picked[pl.ds(1, LANES, stride=2), :].astype(values_out.dtype)


def repeat_kernel(tok_ref, out_ref):
    for i in range(out_ref.shape[0]):
        out_ref[i] = tok_ref[...]


def chunks_of(count):
    return (count + LANES - 1) // LANES


def pick_kernel(
    x_ref,
    rows_ref,
    count_ref,
    place_ref,
    gate_ref,
    key_ref,
    value_ref,
    count_out,
    place_out,
    gate_out,
    keys_out,
    values_out,
    wide,
    took,
):
    n_ep = count_ref.shape[0]
    n_z = n_ep // X
    chunks = place_ref.shape[0] // n_ep
    widen(key_ref, wide, 0)
    widen(value_ref, wide, 1)

    def block(i, carry):
        z = i // X
        shift = (x_ref[0] + X - i % X) % X
        slot = (shift // 2 + (shift % 2) * 2) * n_z + z
        count_out[slot] = count_ref[i]
        for c in range(chunks):
            place_out[pl.ds(slot * chunks + c, 1), :] = place_ref[pl.ds(i * chunks + c, 1), :]
            gate_out[pl.ds(slot * chunks + c, 1), :] = gate_ref[pl.ds(i * chunks + c, 1), :]

        def chunk(c, inner):
            take_rows(
                rows_ref, i * chunks + c, wide, took, keys_out, values_out, slot * chunks + c
            )
            return inner

        lax.fori_loop(0, chunks_of(count_ref[i]), chunk, 0)
        return carry

    lax.fori_loop(0, n_ep, block, 0)


def score_kernel(count_ref, place_ref, keys_ref, *refs, members):
    toks = dict(zip(members, refs))
    out_ref = refs[-1]
    n_z, tok, _ = refs[0].shape
    chunks = place_ref.shape[0] // (X * n_z)
    if len(refs) > len(members) + 1:
        out_ref[...] = refs[-2][...]
    else:
        out_ref[...] = jnp.zeros(out_ref.shape, jnp.float32)
    token_of = lax.broadcasted_iota(jnp.int32, (tok, LANES), 0)

    def line_scores(tokens, line):
        prod = lax.dot_general(
            tokens, keys_ref[line], (((1,), (1,)), ((), ())), preferred_element_type=jnp.float32
        )
        here = place_ref[pl.ds(line, 1), :] == token_of
        return jnp.sum(jnp.where(here, prod, 0.0), axis=0, keepdims=True)

    per = 2

    def first(step, carry):
        jobs = [(g, step * per + j) for j in range(per) for g in members]
        found = [line_scores(toks[g][z], (g * n_z + z) * chunks) for g, z in jobs]
        for (g, z), value in zip(jobs, found):
            out_ref[pl.ds((g * n_z + z) * chunks, 1), :] = value
        return carry

    lax.fori_loop(0, n_z // per, first, 0)

    def more(z, carry):
        for g in members:

            def chunk(c, inner, g=g):
                line = (g * n_z + z) * chunks + c
                out_ref[pl.ds(line, 1), :] = line_scores(toks[g][z], line)
                return inner

            lax.fori_loop(1, chunks_of(count_ref[g * n_z + z]), chunk, 0)
        return carry

    lax.fori_loop(0, n_z, more, 0)


def combine_kernel(count_ref, place_ref, hidden_ref, values_ref, out_ref, acc, *, group):
    n_z, tok, _ = out_ref.shape
    chunks = place_ref.shape[0] // (X * n_z)
    token_of = lax.broadcasted_iota(jnp.int32, (tok, LANES), 0)

    def line_mix(z, c):
        line = (group * n_z + z) * chunks + c
        here = place_ref[pl.ds(line, 1), :] == token_of
        weight = jnp.where(here, hidden_ref[pl.ds(line, 1), :], 0.0)
        high = weight.astype(jnp.bfloat16)
        low = (weight - high.astype(jnp.float32)).astype(jnp.bfloat16)
        rows = values_ref[z * chunks + c]
        return jnp.dot(
            jnp.concatenate([high, low], axis=1),
            jnp.concatenate([rows, rows], axis=0),
            preferred_element_type=jnp.float32,
        )

    def first(half, carry):
        zs = [half * 4 + j for j in range(4)]
        found = [line_mix(z, 0) for z in zs]
        for z, value in zip(zs, found):
            acc[z] = value
        return carry

    lax.fori_loop(0, n_z // 4, first, 0)

    def more(z, carry):
        def chunk(c, inner):
            acc[z] += line_mix(z, c)
            return inner

        lax.fori_loop(1, chunks_of(count_ref[group * n_z + z]), chunk, 0)
        out_ref[z] = acc[z].astype(out_ref.dtype)
        return carry

    lax.fori_loop(0, n_z, more, 0)


def vmem():
    return pl.BlockSpec(memory_space=pltpu.VMEM)


def made(shape, dtype):
    return jax.ShapeDtypeStruct(shape, dtype) if INTERPRET else pltpu.VMEM(shape, dtype)


def stored(shape, dtype):
    return jax.ShapeDtypeStruct(shape, dtype) if INTERPRET else pltpu.HBM(shape, dtype)


def held(value, where=pltpu.VMEM):
    return value if INTERPRET else pltpu.with_memory_space_constraint(value, where)


def smem():
    return pl.BlockSpec(memory_space=pltpu.SMEM)


def to_each(value, axis):
    return lax.all_to_all(
        jnp.broadcast_to(value[None], (lax.axis_size(axis), *value.shape)), axis, 0, 0, tiled=True
    )


def around(shift):
    return [(i, (i + shift) % X) for i in range(X)]


def body(tokens, row_ids, row_gates, key_table, value_table, norm_gain):
    tok, width = tokens.shape
    picks = row_ids.shape[1]
    exp_dev = key_table.shape[0]
    n_ep = lax.axis_size(EP)
    cap = 3 * tok * picks // n_ep
    chunks = cap // LANES
    shift = exp_dev.bit_length() - 1
    lines = n_ep * chunks

    copies = pl.pallas_call(
        repeat_kernel,
        out_shape=made((lax.axis_size("z"), tok, width), tokens.dtype),
        in_specs=[vmem()],
        out_specs=vmem(),
        interpret=INTERPRET,
        compiler_params=pltpu.CompilerParams(vmem_limit_bytes=ROOM),
        name="repeat",
    )(held(tokens, pltpu.HBM))
    near = lax.all_to_all(copies, "z", 0, 0, tiled=True)
    groups = [near]
    for g in (1, 2, 3):
        groups.append(lax.ppermute(near, "x", around(SHIFTS[g])))
    listed = pl.pallas_call(
        lambda *refs: bucket_kernel(*refs, n_ep=n_ep, cap=cap, shift=shift),
        out_shape=jax.ShapeDtypeStruct((n_ep, 8, LANES), jnp.float32),
        in_specs=[vmem(), vmem()],
        out_specs=vmem(),
        scratch_shapes=[
            pltpu.VMEM((6 * n_ep, tok * picks), jnp.bfloat16),
            pltpu.VMEM((cap, tok * picks), jnp.bfloat16),
        ],
        interpret=INTERPRET,
        compiler_params=pltpu.CompilerParams(vmem_limit_bytes=ROOM),
        name="bucket",
    )(row_ids.T, row_gates.T)
    listed = lax.all_to_all(listed, EP, 0, 0, tiled=True)
    codes = listed[:, :chunks].astype(jnp.int32)
    gates = listed[:, chunks : 2 * chunks].reshape(lines, LANES)
    rows = ((codes & (exp_dev - 1)) * 2).reshape(lines, LANES)
    place = ((codes >> shift) - 1).reshape(lines, LANES)
    count = jnp.sum((codes > 0).astype(jnp.int32), axis=(1, 2))

    n_z = n_ep // X
    picked = made((lines, LANES, width), jnp.bfloat16)
    count, place, gates, keys, values = pl.pallas_call(
        pick_kernel,
        out_shape=(
            jax.ShapeDtypeStruct((n_ep,), jnp.int32),
            jax.ShapeDtypeStruct((lines, LANES), jnp.int32),
            jax.ShapeDtypeStruct((lines, LANES), jnp.float32),
            picked,
            stored((lines, LANES, width), jnp.bfloat16),
        ),
        in_specs=[smem(), smem(), smem(), vmem(), vmem(), vmem(), vmem()],
        out_specs=(smem(), vmem(), vmem(), vmem(), vmem()),
        scratch_shapes=[
            pltpu.VMEM((2 * exp_dev, width), jnp.float32),
            pltpu.VMEM((2 * LANES, width), jnp.float32),
        ],
        interpret=INTERPRET,
        compiler_params=pltpu.CompilerParams(vmem_limit_bytes=ROOM),
        name="pick",
    )(
        lax.axis_index("x").reshape(1),
        rows,
        count,
        place,
        gates,
        held(key_table, pltpu.HBM),
        held(value_table, pltpu.HBM),
    )

    def scored(members, *before):
        toks = [held(groups[g]) for g in members]
        return pl.pallas_call(
            lambda *refs: score_kernel(*refs, members=members),
            out_shape=made((lines, LANES), jnp.float32),
            in_specs=[smem()] + [vmem()] * (2 + len(toks) + len(before)),
            out_specs=vmem(),
            interpret=INTERPRET,
            compiler_params=pltpu.CompilerParams(vmem_limit_bytes=ROOM),
            name="score",
        )(count, held(place), held(keys), *toks, *before)

    partial_score = scored((0, 1))
    partial_score = scored((2, 3), held(partial_score))
    score = jnp.sum(lax.all_gather(partial_score, TP), axis=0)
    hidden = jnp.where(place >= 0, jax.nn.gelu(score, approximate=False) * gates, 0.0)

    def combine(group):
        return pl.pallas_call(
            lambda *refs: combine_kernel(*refs, group=group),
            out_shape=made((n_z, tok, width), jnp.bfloat16),
            grid=(1,),
            in_specs=[
                smem(),
                vmem(),
                vmem(),
                pl.BlockSpec((n_z * chunks, LANES, width), lambda i: (group, 0, 0)),
            ],
            out_specs=vmem(),
            scratch_shapes=[pltpu.VMEM((n_z, tok, width), jnp.float32)],
            interpret=INTERPRET,
            compiler_params=pltpu.CompilerParams(vmem_limit_bytes=ROOM),
            name="combine",
        )(count, held(place), held(hidden), held(values, pltpu.HBM))

    parts = []
    for g in (2, 3, 1, 0):
        part = combine(g)
        if g:
            part = lax.ppermute(part, "x", around(-SHIFTS[g]))
        parts.append(part)
    mine = sum(p.astype(jnp.float32) for p in parts).astype(jnp.bfloat16)
    back = lax.all_to_all(mine, "z", 0, 0, tiled=True)
    mixed = jnp.sum(back.astype(jnp.float32), axis=0)
    part = jnp.sum(mixed * mixed, axis=1).reshape(tok // LANES, LANES)
    squares = jnp.sum(to_each(part, TP), axis=0).reshape(tok)
    strength = squares / D
    return (mixed * lax.rsqrt(strength + 1e-06)[:, None] * norm_gain).astype(jnp.bfloat16)


def solution(mesh):
    ep, tp = mesh.devices.shape
    fine = Mesh(mesh.devices.reshape(Z, ep // Z, tp // 2, 2), ("z", "x", "y", "core"))
    in_specs = (P(EP, TP), P(EP, None), P(EP, None), P(EP, TP), P(EP, TP), P(TP))

    return jax.shard_map(body, mesh=fine, in_specs=in_specs, out_specs=P(EP, TP), check_vma=False)
```

```python
import jax
import jax.numpy as jnp
from jax import lax
from jax.experimental import pallas as pl
from jax.experimental.pallas import tpu as pltpu
from jax.sharding import Mesh
from jax.sharding import PartitionSpec as P

D = 2048
LANES = 128
INTERPRET = False
Z = 8
X = 4
ROOM = 24 * 1024 * 1024
SHIFTS = (0, 2, 1, 3)
EP = ("z", "x")
TP = ("y", "core")


def bucket_kernel(ids_ref, gates_ref, out_ref, a_ref, b_ref, *, n_ep, cap, shift):
    picks, tok = ids_ref.shape
    before = jnp.where(
        lax.broadcasted_iota(jnp.int32, (tok, tok), 0)
        < lax.broadcasted_iota(jnp.int32, (tok, tok), 1),
        1.0,
        0.0,
    ).astype(jnp.bfloat16)
    token_no = (lax.broadcasted_iota(jnp.int32, (1, tok), 1) + 1).astype(jnp.float32)
    owners = lax.broadcasted_iota(jnp.int32, (n_ep, tok), 0)
    slots = lax.broadcasted_iota(jnp.int32, (cap, tok), 0)
    base = jnp.zeros((n_ep, 1), jnp.float32)
    for k in range(picks):
        ids = ids_ref[k : k + 1, :]
        mine = (ids >> shift) == owners
        hot = jnp.where(mine, 1.0, 0.0)
        rank = base + jnp.dot(
            hot.astype(jnp.bfloat16), before, preferred_element_type=jnp.float32
        )
        place = jnp.sum(jnp.where(mine, rank, 0.0), axis=0, keepdims=True).astype(jnp.int32)
        base = base + jnp.sum(hot, axis=1, keepdims=True)
        b_ref[:, k * tok : (k + 1) * tok] = jnp.where(slots == place, 1.0, 0.0).astype(
            jnp.bfloat16
        )
        local = ids & ((1 << shift) - 1)
        gate = gates_ref[k : k + 1, :]
        gate_hi = gate.astype(jnp.bfloat16).astype(jnp.float32)
        gate_mid = (gate - gate_hi).astype(jnp.bfloat16).astype(jnp.float32)
        gate_lo = gate - gate_hi - gate_mid
        values = (
            token_no,
            (local >> 4).astype(jnp.float32),
            (local & 15).astype(jnp.float32),
            gate_hi,
            gate_mid,
            gate_lo,
        )
        for c, value in enumerate(values):
            a_ref[c * n_ep : (c + 1) * n_ep, k * tok : (k + 1) * tok] = jnp.where(
                mine, value, 0.0
            ).astype(jnp.bfloat16)
    res = lax.dot_general(
        a_ref[...], b_ref[...], (((1,), (1,)), ((), ())), preferred_element_type=jnp.float32
    )
    part = [res[c * n_ep : (c + 1) * n_ep] for c in range(6)]
    code = part[0] * float(1 << shift) + (part[1] * 16.0 + part[2])
    gates = part[3] + part[4] + part[5]
    chunks = cap // LANES
    out_ref[...] = jnp.zeros(out_ref.shape, jnp.float32)
    for j in range(chunks):
        out_ref[:, j, :] = code[:, j * LANES : (j + 1) * LANES]
        out_ref[:, chunks + j, :] = gates[:, j * LANES : (j + 1) * LANES]


def widen(table_ref, wide_ref, which):
    step = 256

    def one(i, carry):
        rows = pl.ds(pl.multiple_of(i * step, step), step)
        into = pl.ds(pl.multiple_of(i * 2 * step, 2 * step) + which, step, stride=2)
        wide_ref[into, :] = table_ref[rows, :].astype(jnp.float32)
        return carry

    lax.fori_loop(0, table_ref.shape[0] // step, one, 0)


def take_rows(rows_ref, line, wide_ref, picked, keys_out, values_out, to):
    for s in range(LANES):
        at = pl.multiple_of(rows_ref[line, s], 2)
        picked[pl.ds(2 * s, 2), :] = wide_ref[pl.ds(at, 2), :]
    keys_out[to] = picked[pl.ds(0, LANES, stride=2), :].astype(keys_out.dtype)
    values_out[to] = picked[pl.ds(1, LANES, stride=2), :].astype(values_out.dtype)


def repeat_kernel(tok_ref, out_ref):
    for i in range(out_ref.shape[0]):
        out_ref[i] = tok_ref[...]


def chunks_of(count):
    return (count + LANES - 1) // LANES


def pick_kernel(
    x_ref,
    rows_ref,
    count_ref,
    place_ref,
    gate_ref,
    key_ref,
    value_ref,
    count_out,
    place_out,
    gate_out,
    keys_out,
    values_out,
    wide,
    took,
):
    n_ep = count_ref.shape[0]
    n_z = n_ep // X
    chunks = place_ref.shape[0] // n_ep
    widen(key_ref, wide, 0)
    widen(value_ref, wide, 1)

    def block(i, carry):
        z = i // X
        shift = (x_ref[0] + X - i % X) % X
        slot = (shift // 2 + (shift % 2) * 2) * n_z + z
        count_out[slot] = count_ref[i]
        for c in range(chunks):
            place_out[pl.ds(slot * chunks + c, 1), :] = place_ref[pl.ds(i * chunks + c, 1), :]
            gate_out[pl.ds(slot * chunks + c, 1), :] = gate_ref[pl.ds(i * chunks + c, 1), :]

        def chunk(c, inner):
            take_rows(
                rows_ref, i * chunks + c, wide, took, keys_out, values_out, slot * chunks + c
            )
            return inner

        lax.fori_loop(0, chunks_of(count_ref[i]), chunk, 0)
        return carry

    lax.fori_loop(0, n_ep, block, 0)


def score_kernel(count_ref, place_ref, keys_ref, *refs, members):
    toks = dict(zip(members, refs))
    out_ref = refs[-1]
    n_z, tok, _ = refs[0].shape
    chunks = place_ref.shape[0] // (X * n_z)
    if len(refs) > len(members) + 1:
        out_ref[...] = refs[-2][...]
    else:
        out_ref[...] = jnp.zeros(out_ref.shape, jnp.float32)
    token_of = lax.broadcasted_iota(jnp.int32, (tok, LANES), 0)

    def line_scores(tokens, line):
        prod = lax.dot_general(
            tokens, keys_ref[line], (((1,), (1,)), ((), ())), preferred_element_type=jnp.float32
        )
        here = place_ref[pl.ds(line, 1), :] == token_of
        return jnp.sum(jnp.where(here, prod, 0.0), axis=0, keepdims=True)

    per = 4

    def first(step, carry):
        jobs = [(g, step * per + j) for j in range(per) for g in members]
        found = [line_scores(toks[g][z], (g * n_z + z) * chunks) for g, z in jobs]
        for (g, z), value in zip(jobs, found):
            out_ref[pl.ds((g * n_z + z) * chunks, 1), :] = value
        return carry

    lax.fori_loop(0, n_z // per, first, 0)

    def more(z, carry):
        for g in members:

            def chunk(c, inner, g=g):
                line = (g * n_z + z) * chunks + c
                out_ref[pl.ds(line, 1), :] = line_scores(toks[g][z], line)
                return inner

            lax.fori_loop(1, chunks_of(count_ref[g * n_z + z]), chunk, 0)
        return carry

    lax.fori_loop(0, n_z, more, 0)


def combine_kernel(count_ref, place_ref, hidden_ref, values_ref, out_ref, acc, *, group):
    n_z, tok, _ = out_ref.shape
    chunks = place_ref.shape[0] // (X * n_z)
    token_of = lax.broadcasted_iota(jnp.int32, (tok, LANES), 0)

    def line_mix(z, c):
        line = (group * n_z + z) * chunks + c
        here = place_ref[pl.ds(line, 1), :] == token_of
        weight = jnp.where(here, hidden_ref[pl.ds(line, 1), :], 0.0)
        high = weight.astype(jnp.bfloat16)
        low = (weight - high.astype(jnp.float32)).astype(jnp.bfloat16)
        rows = values_ref[z * chunks + c]
        return jnp.dot(
            jnp.concatenate([high, low], axis=1),
            jnp.concatenate([rows, rows], axis=0),
            preferred_element_type=jnp.float32,
        )

    def first(half, carry):
        zs = [half * 4 + j for j in range(4)]
        found = [line_mix(z, 0) for z in zs]
        for z, value in zip(zs, found):
            acc[z] = value
        return carry

    lax.fori_loop(0, n_z // 4, first, 0)

    def more(z, carry):
        def chunk(c, inner):
            acc[z] += line_mix(z, c)
            return inner

        lax.fori_loop(1, chunks_of(count_ref[group * n_z + z]), chunk, 0)
        out_ref[z] = acc[z].astype(out_ref.dtype)
        return carry

    lax.fori_loop(0, n_z, more, 0)


def vmem():
    return pl.BlockSpec(memory_space=pltpu.VMEM)


def made(shape, dtype):
    return jax.ShapeDtypeStruct(shape, dtype) if INTERPRET else pltpu.VMEM(shape, dtype)


def held(value, where=pltpu.VMEM):
    return value if INTERPRET else pltpu.with_memory_space_constraint(value, where)


def smem():
    return pl.BlockSpec(memory_space=pltpu.SMEM)


def to_each(value, axis):
    return lax.all_to_all(
        jnp.broadcast_to(value[None], (lax.axis_size(axis), *value.shape)), axis, 0, 0, tiled=True
    )


def around(shift):
    return [(i, (i + shift) % X) for i in range(X)]


def body(tokens, row_ids, row_gates, key_table, value_table, norm_gain):
    tok, width = tokens.shape
    picks = row_ids.shape[1]
    exp_dev = key_table.shape[0]
    n_ep = lax.axis_size(EP)
    cap = 3 * tok * picks // n_ep
    chunks = cap // LANES
    shift = exp_dev.bit_length() - 1
    lines = n_ep * chunks

    copies = pl.pallas_call(
        repeat_kernel,
        out_shape=made((lax.axis_size("z"), tok, width), tokens.dtype),
        in_specs=[vmem()],
        out_specs=vmem(),
        interpret=INTERPRET,
        compiler_params=pltpu.CompilerParams(vmem_limit_bytes=ROOM),
        name="repeat",
    )(held(tokens, pltpu.HBM))
    near = lax.all_to_all(copies, "z", 0, 0, tiled=True)
    groups = [near]
    for g in (1, 2, 3):
        groups.append(lax.ppermute(near, "x", around(SHIFTS[g])))
    listed = pl.pallas_call(
        lambda *refs: bucket_kernel(*refs, n_ep=n_ep, cap=cap, shift=shift),
        out_shape=jax.ShapeDtypeStruct((n_ep, 8, LANES), jnp.float32),
        in_specs=[vmem(), vmem()],
        out_specs=vmem(),
        scratch_shapes=[
            pltpu.VMEM((6 * n_ep, tok * picks), jnp.bfloat16),
            pltpu.VMEM((cap, tok * picks), jnp.bfloat16),
        ],
        interpret=INTERPRET,
        compiler_params=pltpu.CompilerParams(vmem_limit_bytes=ROOM),
        name="bucket",
    )(row_ids.T, row_gates.T)
    listed = lax.all_to_all(listed, EP, 0, 0, tiled=True)
    codes = listed[:, :chunks].astype(jnp.int32)
    gates = listed[:, chunks : 2 * chunks].reshape(lines, LANES)
    rows = ((codes & (exp_dev - 1)) * 2).reshape(lines, LANES)
    place = ((codes >> shift) - 1).reshape(lines, LANES)
    count = jnp.sum((codes > 0).astype(jnp.int32), axis=(1, 2))

    n_z = n_ep // X
    picked = made((lines, LANES, width), jnp.bfloat16)
    count, place, gates, keys, values = pl.pallas_call(
        pick_kernel,
        out_shape=(
            jax.ShapeDtypeStruct((n_ep,), jnp.int32),
            jax.ShapeDtypeStruct((lines, LANES), jnp.int32),
            jax.ShapeDtypeStruct((lines, LANES), jnp.float32),
            picked,
            jax.ShapeDtypeStruct(picked.shape, picked.dtype),
        ),
        in_specs=[smem(), smem(), smem(), vmem(), vmem(), vmem(), vmem()],
        out_specs=(smem(), vmem(), vmem(), vmem(), vmem()),
        scratch_shapes=[
            pltpu.VMEM((2 * exp_dev, width), jnp.float32),
            pltpu.VMEM((2 * LANES, width), jnp.float32),
        ],
        interpret=INTERPRET,
        compiler_params=pltpu.CompilerParams(vmem_limit_bytes=ROOM),
        name="pick",
    )(
        lax.axis_index("x").reshape(1),
        rows,
        count,
        place,
        gates,
        held(key_table, pltpu.HBM),
        held(value_table, pltpu.HBM),
    )

    def scored(members, *before):
        toks = [held(groups[g]) for g in members]
        return pl.pallas_call(
            lambda *refs: score_kernel(*refs, members=members),
            out_shape=made((lines, LANES), jnp.float32),
            in_specs=[smem()] + [vmem()] * (2 + len(toks) + len(before)),
            out_specs=vmem(),
            interpret=INTERPRET,
            compiler_params=pltpu.CompilerParams(vmem_limit_bytes=ROOM),
            name="score",
        )(count, held(place), held(keys), *toks, *before)

    partial_score = scored((0, 1))
    partial_score = scored((2, 3), held(partial_score))
    score = jnp.sum(lax.all_gather(partial_score, TP), axis=0)
    hidden = jnp.where(place >= 0, jax.nn.gelu(score, approximate=False) * gates, 0.0)

    def combine(group):
        return pl.pallas_call(
            lambda *refs: combine_kernel(*refs, group=group),
            out_shape=made((n_z, tok, width), jnp.bfloat16),
            grid=(1,),
            in_specs=[
                smem(),
                vmem(),
                vmem(),
                pl.BlockSpec((n_z * chunks, LANES, width), lambda i: (group, 0, 0)),
            ],
            out_specs=vmem(),
            scratch_shapes=[pltpu.VMEM((n_z, tok, width), jnp.float32)],
            interpret=INTERPRET,
            compiler_params=pltpu.CompilerParams(vmem_limit_bytes=ROOM),
            name="combine",
        )(count, held(place), held(hidden), held(values, pltpu.HBM))

    parts = []
    for g in (1, 2, 3, 0):
        part = combine(g)
        if g:
            part = lax.ppermute(part, "x", around(-SHIFTS[g]))
        parts.append(part)
    mine = sum(p.astype(jnp.float32) for p in parts).astype(jnp.bfloat16)
    back = lax.all_to_all(mine, "z", 0, 0, tiled=True)
    mixed = jnp.sum(back.astype(jnp.float32), axis=0)
    part = jnp.sum(mixed * mixed, axis=1).reshape(tok // LANES, LANES)
    squares = jnp.sum(to_each(part, TP), axis=0).reshape(tok)
    strength = squares / D
    return (mixed * lax.rsqrt(strength + 1e-06)[:, None] * norm_gain).astype(jnp.bfloat16)


def solution(mesh):
    ep, tp = mesh.devices.shape
    fine = Mesh(mesh.devices.reshape(Z, ep // Z, tp // 2, 2), ("z", "x", "y", "core"))
    in_specs = (P(EP, TP), P(EP, None), P(EP, None), P(EP, TP), P(EP, TP), P(TP))

    return jax.shard_map(body, mesh=fine, in_specs=in_specs, out_specs=P(EP, TP), check_vma=False)
```
